32 devices in a mesh: ep: 8 (over z, x), tp: 4 (over y, core).
Axes of the slice: x: 2, y: 2, z: 4, core: 2. Of those that a mesh axis runs over, the one named last changes fastest.
Arguments:
- queries: bfloat16 [2048, 1024], P('ep', 'tp'), may hold values from -256 to 256
- key_rows: bfloat16 [2048, 1024], P('ep', 'tp'), may hold values from -8 to 8
- value_rows: bfloat16 [2048, 1024], P('ep', 'tp'), may hold values from -6 to 6
- head_lambda: float32 [8], P('tp'), may hold values from 0.3 to 0.8
- sub_gain: float32 [128], replicated, may hold values from 0.1 to 1.9
- out_weight: bfloat16 [1024, 2048], P('tp'), may hold values from -0.1875 to 0.1875
- expert_input: bfloat16 [1536, 2048], P('ep'), may hold values from -6 to 6
- norm_gain: float32 [2048], replicated, may hold values from 0.1 to 1.9
- route_ids: int32 [1536, 2], P('ep'), may hold values from 0 to 7, all different within a row; in each aligned block of 192 rows (0 to 191, 192 to 383, ...) at most 80 rows name the same one
- route_weight: float32 [1536, 2], P('ep'), may hold values from 0.25 to 1
- gate_weight: bfloat16 [8, 2048, 3584], P('ep', None, 'tp'), may hold values from -0.125 to 0.125
- up_weight: bfloat16 [8, 2048, 3584], P('ep', None, 'tp'), may hold values from -0.125 to 0.125
- down_weight: bfloat16 [8, 3584, 2048], P('ep', 'tp'), may hold values from -0.09375 to 0.09375
Outputs:
- mixer_out: bfloat16 [2048, 2048], P(('ep', 'tp'))
- expert_out: bfloat16 [1536, 2048], P('ep', 'tp')
The draws below stay inside these ranges and needn't reach their ends.
Inputs may be any that keep to these rules, and one draw needn't show every extreme that they name: `route_ids`: each row names 2 different experts. In each aligned block of 192 rows no expert is named by more than 80 rows, a bound that some block reaches.
All inputs are finite; a program needn't handle non-finite values.
Results may differ from the reference program's by a relative error of at most 0.014.
Values may be sent and summed in bfloat16 or wider, within the bound.
No kernel may reach another device: no remote copies, remote signals or barrier semaphores. Data moves between devices by JAX's collectives and lax.ppermute only.
A program may use at most 256 MiB of HBM per device.

```python
import math
import jax
import jax.numpy as jnp
import numpy as np
from jax import lax

D = 2048
HEADS = 8
HEAD_DIM = 64
VALUE_DIM = 128
FF = 3584
TOP = 2
TOK_B_DEV = 192
EXPERTS = 8
CAP = 80
TOKENS_A = 2048
TOKENS_B = 1536
N_EP = 8
N_TP = 4


def query_key_pair(key):
    base = jax.random.fold_in(key, 11)
    key_draw, query_draw = jax.random.split(base, 2)
    shape = (TOKENS_A, HEADS, 2, HEAD_DIM)
    key_vals = 1.3 * jax.random.truncated_normal(key_draw, -6.0, 6.0, shape, jnp.float32)
    query_vals = 1.3 * jax.random.truncated_normal(query_draw, -6.0, 6.0, shape, jnp.float32)
    return (query_vals.reshape(TOKENS_A, HEADS * 2 * HEAD_DIM), key_vals.reshape(TOKENS_A, HEADS * 2 * HEAD_DIM))


def draw_queries(key, part):
    return query_key_pair(key)[0].astype(jnp.bfloat16)


def draw_key_rows(key, part):
    return query_key_pair(key)[1].astype(jnp.bfloat16)


def block_scale(stream_key, dims, cuts, smallest, largest):
    loudness, own = 1.0, jax.random.fold_in(stream_key, 6)
    for position, parts in cuts:
        draws = jnp.exp(jax.random.uniform(jax.random.fold_in(own, position), (parts,), jnp.float32, smallest / len(cuts), largest / len(cuts)))
        loudness = loudness * jnp.repeat(draws, dims[position] // parts).reshape([-1 if axis == position else 1 for axis in range(len(dims))])
    return loudness


def shared_out(stream_key, own, number, rows, count, top, limit, skew):
    order = jax.random.permutation(stream_key, count)
    heavy_load, usual = portions_of(count, rows * top, limit, skew, True), portions_of(count, rows * top, limit, skew, False)
    places = jnp.arange(count)

    def named(lengths, offset_by):
        used = int((lengths > 0).sum())
        fixed = max(1, used // 4)
        passed = fixed + (places - fixed + offset_by * (used - fixed)) % max(1, count - fixed)
        return jnp.zeros((count,), jnp.int32).at[order[jnp.where(places < fixed, places, passed)]].set(jnp.asarray(lengths, jnp.int32))

    lengths = jnp.where(number % 4 == 0, named(heavy_load, number // 4), named(usual, number - number // 4 - 1))
    mixed = jax.random.permutation(jax.random.fold_in(own, 3), count)
    source_of, receiver = mixed[0:count // 2 * 2:2], mixed[1:count // 2 * 2:2]
    slack = jnp.minimum(lengths[source_of] - 1, limit - lengths[receiver]) // 2
    slack = jnp.where((source_of == order[0]) | (receiver == order[0]) | (lengths[receiver] == 0), 0, jnp.maximum(slack, 0))
    passed = jax.random.randint(jax.random.fold_in(own, 4), (count // 2,), 0, 1 << 20) % (slack + 1)
    lengths = lengths.at[source_of].add(-passed).at[receiver].add(passed)
    items = jnp.searchsorted(jnp.cumsum(lengths), jnp.arange(rows * top), side="right").astype(jnp.int32)
    grid = items.reshape(top, rows).T
    grid = grid[jax.random.permutation(jax.random.fold_in(own, 1), rows)]
    offset_by = jax.random.randint(jax.random.fold_in(own, 2), (rows, 1), 0, top)
    return jnp.take_along_axis(grid, (jnp.arange(top)[None, :] + offset_by) % top, axis=1)


def portions_of(amount, total, limit, skew, full):
    loads = [(1 << 20) // math.isqrt(standing ** skew) + 1 for standing in range(1, amount + 1)]
    largest = limit if full else min(limit, max(-(-total // amount), total * loads[0] // sum(loads)))
    least = 1 if total - largest >= amount - 1 else 0
    holding, rest = [largest] + [least] * (amount - 1), total - largest - least * (amount - 1)
    while rest > 0:
        free = [i for i in range(1, amount) if holding[i] < largest] or [i for i in range(1, amount) if holding[i] < limit]
        whole, budget = sum([loads[i] for i in free]), rest
        for i in free:
            addition = min(limit - holding[i], max(1, budget * loads[i] // whole), rest)
            holding[i] = holding[i] + addition
            rest = rest - addition
    return np.array(holding)


def noise(key, shape, spread, reach, shards=(), kind=jnp.bfloat16):
    level = block_scale(key, shape, shards, -0.22, 0.18) if shards else 1.0
    entries = jax.random.normal(key, shape, jnp.float32) * spread * level
    return jnp.minimum(jnp.maximum(entries, -reach), reach).astype(kind)


def setup_inputs(seed: int = 0) -> dict:
    arg_keys = jax.random.split(jax.random.key(seed), 14)
    queries = draw_queries(jax.random.fold_in(arg_keys[13], 71), 0)
    key_rows = draw_key_rows(jax.random.fold_in(arg_keys[13], 71), 0)
    value_rows = noise(arg_keys[2], (TOKENS_A, HEADS * VALUE_DIM), 1.0, 6.0, ((0, 8), (1, 4)))
    head_lambda = jnp.clip(0.3 + 0.5 * jax.random.uniform(arg_keys[3], (HEADS,), jnp.float32) ** block_scale(arg_keys[3], (HEADS,), ((0, 4),), -0.2, 0.2), 0.3, 0.8)
    sub_gain = jnp.clip(1.0 + 0.18 * jax.random.normal(arg_keys[4], (VALUE_DIM,), jnp.float32), 0.1, 1.9)
    out_weight = noise(arg_keys[5], (HEADS * VALUE_DIM, D), (HEADS * VALUE_DIM) ** -0.5, 0.1875, ((0, 4),))
    expert_input = noise(arg_keys[6], (TOKENS_B, D), 1.0, 6.0, ((0, 8),))
    norm_gain = jnp.clip(1.0 + 0.18 * jax.random.normal(arg_keys[7], (D,), jnp.float32), 0.1, 1.9)
    route_ids_keys = jax.random.split(jax.random.fold_in(arg_keys[8], 1), TOKENS_B // TOK_B_DEV)
    route_ids_turns = jax.random.permutation(jax.random.fold_in(arg_keys[8], 3), TOKENS_B // TOK_B_DEV)
    route_ids = jax.vmap(lambda own, number: shared_out(jax.random.fold_in(arg_keys[8], 2), own, number, TOK_B_DEV, EXPERTS, TOP, CAP, 1))(route_ids_keys, route_ids_turns).reshape((TOKENS_B, TOP))
    route_weight = jnp.clip(0.25 + 0.75 * jax.random.uniform(arg_keys[9], (TOKENS_B, TOP), jnp.float32) ** block_scale(arg_keys[9], (TOKENS_B, TOP), ((0, 8),), -0.2, 0.2), 0.25, 1.0)
    gate_weight = noise(arg_keys[10], (EXPERTS, D, FF), D ** -0.5, 0.125, ((0, 8), (2, 4)))
    up_weight = noise(arg_keys[11], (EXPERTS, D, FF), D ** -0.5, 0.125, ((0, 8), (2, 4)))
    down_weight = noise(arg_keys[12], (EXPERTS, FF, D), FF ** -0.5, 0.09375, ((0, 8), (1, 4)))
    return {"queries": queries, "key_rows": key_rows, "value_rows": value_rows, "head_lambda": head_lambda, "sub_gain": sub_gain, "out_weight": out_weight, "expert_input": expert_input, "norm_gain": norm_gain, "route_ids": route_ids, "route_weight": route_weight, "gate_weight": gate_weight, "up_weight": up_weight, "down_weight": down_weight}


EPS = 1e-06

def round_keep(values):
    return lax.optimization_barrier(values.astype(jnp.bfloat16)).astype(jnp.float32)

def head_output(query_head, key_head, value_head, lam_value, sub_gain):
    block_rows = math.gcd(TOKENS_A, 512)
    scaling = HEAD_DIM ** (-0.5)
    key_pos = jnp.arange(TOKENS_A, dtype=jnp.int32)
    key_wide = key_head.astype(jnp.float32)
    value_wide = value_head.astype(jnp.float32)

    def one_block(block_index):
        first_row = (block_index * block_rows).astype(jnp.int32)
        query_block = lax.dynamic_slice_in_dim(query_head, first_row, block_rows, 0).astype(jnp.float32)
        scores = jnp.einsum('qmd,kmd->mqk', query_block, key_wide) * scaling
        query_pos = first_row + jnp.arange(block_rows, dtype=jnp.int32)
        allowed = query_pos[:, None] >= key_pos[None, :]
        scores = jnp.where(allowed, scores, -jnp.inf)
        row_max = lax.optimization_barrier(jnp.max(scores, axis=-1, keepdims=True))
        weights = jnp.where(allowed, jnp.exp(scores - row_max), 0.0)
        row_total = lax.optimization_barrier(jnp.sum(weights, axis=-1))
        numerator = jnp.einsum('mqk,kd->mqd', round_keep(weights), value_wide)
        per_map = numerator / row_total[..., None]
        contrast = per_map[0] - lam_value * per_map[1]
        normed = contrast * lax.rsqrt(lax.optimization_barrier(jnp.mean(contrast * contrast, axis=-1, keepdims=True)) + EPS) * sub_gain
        return normed.astype(jnp.bfloat16)
    blocks = lax.map(one_block, jnp.arange(TOKENS_A // block_rows, dtype=jnp.int32))
    return blocks.reshape(TOKENS_A, VALUE_DIM)

def reference(queries, key_rows, value_rows, head_lambda, sub_gain, out_weight, expert_input, norm_gain, route_ids, route_weight, gate_weight, up_weight, down_weight):
    query_heads = jnp.moveaxis(queries.reshape(TOKENS_A, HEADS, 2, HEAD_DIM), 1, 0)
    key_heads = jnp.moveaxis(key_rows.reshape(TOKENS_A, HEADS, 2, HEAD_DIM), 1, 0)
    value_heads = jnp.moveaxis(value_rows.reshape(TOKENS_A, HEADS, VALUE_DIM), 1, 0)

    def per_head(operands):
        return head_output(operands[0], operands[1], operands[2], operands[3], sub_gain)
    attended = lax.map(per_head, (query_heads, key_heads, value_heads, head_lambda))
    attended = jnp.moveaxis(attended, 0, 1).reshape(TOKENS_A, HEADS * VALUE_DIM)
    group_cols = HEADS // N_TP * VALUE_DIM
    mixed_sum = jnp.zeros((TOKENS_A, D), jnp.float32)
    for group_index in range(N_TP):
        lower = group_index * group_cols
        share = jnp.dot(attended[:, lower:lower + group_cols], out_weight[lower:lower + group_cols], preferred_element_type=jnp.float32)
        mixed_sum = mixed_sum + round_keep(share)
    mixer_out = mixed_sum.astype(jnp.bfloat16)
    wide_rows = expert_input.astype(jnp.float32)
    normed_input = (wide_rows * lax.rsqrt(lax.optimization_barrier(jnp.mean(wide_rows * wide_rows, axis=-1, keepdims=True)) + EPS) * norm_gain).astype(jnp.bfloat16)
    flat_ids = route_ids.reshape(N_EP, TOK_B_DEV * TOP)
    onehot = (flat_ids[..., None] == jnp.arange(EXPERTS, dtype=jnp.int32)).astype(jnp.int32)
    rank_before = jnp.cumsum(onehot, axis=1) - onehot
    slot_index = lax.optimization_barrier(jnp.sum(rank_before * onehot, axis=-1))
    source = jnp.arange(N_EP, dtype=jnp.int32)[:, None]
    buffer_pos = ((flat_ids * N_EP + source) * CAP + slot_index).astype(jnp.int32)
    token_index = (source * TOK_B_DEV + jnp.arange(TOK_B_DEV * TOP, dtype=jnp.int32)[None, :] // TOP).astype(jnp.int32)
    row_table = jnp.full((EXPERTS * N_EP * CAP,), TOKENS_B, jnp.int32)
    row_table = row_table.at[buffer_pos.reshape(-1)].set(token_index.reshape(-1))
    padded = jnp.concatenate([normed_input, jnp.zeros((1, D), jnp.bfloat16)], axis=0)
    unit_share = FF // N_TP

    def one_expert(operands):
        gathered = padded[operands[0]]
        gate_act = jnp.dot(gathered, operands[1], preferred_element_type=jnp.float32)
        up_act = jnp.dot(gathered, operands[2], preferred_element_type=jnp.float32)
        hidden = (jax.nn.silu(gate_act) * up_act).astype(jnp.bfloat16)
        result_sum = jnp.zeros((N_EP * CAP, D), jnp.float32)
        for group_index in range(N_TP):
            lower = group_index * unit_share
            share = jnp.dot(hidden[:, lower:lower + unit_share], operands[3][lower:lower + unit_share], preferred_element_type=jnp.float32)
            result_sum = result_sum + round_keep(share)
        return result_sum.astype(jnp.bfloat16)
    results = lax.map(one_expert, (row_table.reshape(EXPERTS, N_EP * CAP), gate_weight, up_weight, down_weight))
    picked = results.reshape(EXPERTS * N_EP * CAP, D)[buffer_pos.reshape(-1)]
    picked = picked.reshape(TOKENS_B, TOP, D).astype(jnp.float32)
    expert_out = lax.optimization_barrier(jnp.sum(picked * route_weight[..., None], axis=1)).astype(jnp.bfloat16)
    return (mixer_out, expert_out)
```

```python
import functools

import jax
import jax.numpy as jnp
from jax import lax
from jax.experimental import pallas as pl
from jax.experimental.pallas import tpu as pltpu
from jax.sharding import PartitionSpec as P

EPS = 1e-06
F32 = jnp.float32
BF16 = jnp.bfloat16


def swap(x, axis, mask):
    count = lax.axis_size(axis)
    return lax.ppermute(x, axis, [(i, i ^ mask) for i in range(count)])


def later(x, axis, step):
    count = lax.axis_size(axis)
    return lax.ppermute(x, axis, [(i, i + step) for i in range(count - step)])


def gathered_keys(key_rows, value_rows):
    rows_here, width = key_rows.shape
    count = lax.axis_size("ep")
    own = jnp.concatenate([key_rows, value_rows], axis=1)
    here = lax.axis_index("ep")
    if count > 8 or count % 2:
        both = lax.all_gather(own, "ep", axis=0, tiled=True)
        return both, jnp.arange(count, dtype=jnp.int32)
    pieces = [own] + [later(own, "ep", 2 * k) for k in range(1, count // 2)]
    line = jnp.concatenate(pieces, axis=0)
    other = swap(line, "ep", 1)
    steps = 2 * jnp.arange(count // 2, dtype=jnp.int32)
    places = jnp.concatenate([here - steps, (here ^ 1) - steps])
    return jnp.concatenate([line, other], axis=0), places


def attention(queries, both, places, head_lambda, sub_gain, out_weight):
    rows_here = queries.shape[0]
    heads_here = head_lambda.shape[0]
    head_width = queries.shape[1] // (2 * heads_here)
    width = queries.shape[1]
    value_width = (both.shape[1] - width) // heads_here
    scaling = head_width ** (-0.5)
    length = both.shape[0]
    query_blocks = queries.reshape(rows_here, heads_here, 2, head_width)
    query_pos = lax.axis_index("ep") * rows_here + jnp.arange(rows_here, dtype=jnp.int32)
    key_pos = (
        places[:, None] * rows_here + jnp.arange(rows_here, dtype=jnp.int32)[None, :]
    ).reshape(length)
    key_blocks = both[:, :width].reshape(length, heads_here, 2, head_width)
    value_blocks = both[:, width:].reshape(length, heads_here, value_width)
    scores = (
        jnp.einsum("qhmd,khmd->hmqk", query_blocks, key_blocks, preferred_element_type=F32)
        * scaling
    )
    allowed = (query_pos[:, None] >= key_pos[None, :]) & (key_pos[None, :] >= 0)
    scores = jnp.where(allowed, scores, -1e30)
    row_max = jnp.max(scores, axis=-1)
    weights = jnp.where(allowed, jnp.exp(scores - row_max[..., None]), 0.0)
    row_total = jnp.sum(weights, axis=-1)
    numerator = jnp.einsum(
        "hmqk,khd->hmqd", weights.astype(BF16), value_blocks, preferred_element_type=F32
    )
    per_map = numerator / row_total[..., None]
    contrast = per_map[:, 0] - head_lambda[:, None, None] * per_map[:, 1]
    normed = (
        contrast * lax.rsqrt(jnp.mean(contrast * contrast, axis=-1, keepdims=True) + EPS) * sub_gain
    ).astype(BF16)
    attended = jnp.transpose(normed, (1, 0, 2)).reshape(rows_here, heads_here * value_width)
    return jnp.dot(attended, out_weight, preferred_element_type=F32).astype(BF16)


def dispatch_kernel(
    experts, capacity, place_ref, ids_ref, rows_ref, gain_ref, out_ref, onehot_ref
):
    rows, width = rows_ref.shape
    cols = out_ref.shape[1]
    first = pl.multiple_of(place_ref[0] * cols, cols)
    wide = rows_ref[...].astype(F32)
    scale = lax.rsqrt(jnp.mean(wide * wide, axis=-1, keepdims=True) + EPS)
    part = rows_ref[:, pl.ds(first, cols)].astype(F32)
    normed = (part * scale * gain_ref[:, pl.ds(first, cols)]).astype(BF16)
    numbers = lax.broadcasted_iota(jnp.int32, (experts, rows), 0)
    named = (ids_ref[0:1, :] == numbers) | (ids_ref[1:2, :] == numbers)
    before = (
        lax.broadcasted_iota(jnp.int32, (rows, rows), 0)
        < lax.broadcasted_iota(jnp.int32, (rows, rows), 1)
    ).astype(F32).astype(BF16)
    rank = jnp.dot(named.astype(F32).astype(BF16), before, preferred_element_type=F32)
    rank = jnp.where(named, rank, -1.0)
    slot = lax.broadcasted_iota(jnp.int32, (capacity, rows), 0).astype(F32)
    for e in range(experts):
        onehot_ref[e * capacity : (e + 1) * capacity, :] = (
            rank[e : e + 1, :] == slot
        ).astype(F32)
    out_ref[...] = jnp.dot(
        onehot_ref[...].astype(BF16), normed, preferred_element_type=F32
    ).astype(BF16)


def dispatched(expert_input, norm_gain, ids_across, capacity):
    rows, width = expert_input.shape
    experts = lax.axis_size("ep")
    cols = width // lax.axis_size("tp")
    slots = experts * capacity
    vmem = pl.BlockSpec(memory_space=pltpu.VMEM)
    return pl.pallas_call(
        functools.partial(dispatch_kernel, experts, capacity),
        out_shape=jax.ShapeDtypeStruct((slots, cols), BF16),
        in_specs=[pl.BlockSpec(memory_space=pltpu.SMEM), vmem, vmem, vmem],
        out_specs=vmem,
        scratch_shapes=[pltpu.VMEM((slots, rows), F32)],
        cost_estimate=pl.CostEstimate(
            flops=2 * slots * rows * cols, bytes_accessed=2 * rows * width, transcendentals=rows
        ),
        name="dispatch",
    )(
        lax.axis_index("tp").astype(jnp.int32).reshape(1),
        ids_across,
        expert_input,
        norm_gain.reshape(1, width),
    )


def ffn_kernel(
    order_ref, x0, x1, x2, x3, gate_ref, up_ref, down_ref, keep_ref, send_ref, acc_g, acc_u, hidden
):
    step = pl.program_id(0)
    for k, x_ref in enumerate((x0, x1, x2, x3)):

        @pl.when(step == k)
        def _(k=k, x_ref=x_ref):
            gate = jnp.dot(x_ref[...], gate_ref[0], preferred_element_type=F32)
            up = jnp.dot(x_ref[...], up_ref[0], preferred_element_type=F32)
            if k:
                gate += acc_g[...]
                up += acc_u[...]
            if k < 3:
                acc_g[...] = gate
                acc_u[...] = up
            else:
                hidden[...] = (gate / (1.0 + jnp.exp(-gate)) * up).astype(BF16)

    @pl.when((step == 4) | (step == 5))
    def _():
        send_ref[...] = jnp.dot(hidden[...], down_ref[0], preferred_element_type=F32).astype(BF16)

    @pl.when(step >= 6)
    def _():
        keep_ref[...] = jnp.dot(hidden[...], down_ref[0], preferred_element_type=F32).astype(BF16)


def ffn(order, pieces, gate_weight, up_weight, down_weight):
    rows, cols = pieces[0].shape
    width, units = gate_weight.shape[1:]

    def clamp(i, low, high):
        return jnp.minimum(jnp.maximum(i, low), high)

    def whole():
        return pl.BlockSpec((rows, cols), lambda i, order: (0, 0))

    def weight_in():
        return pl.BlockSpec((1, cols, units), lambda i, order: (0, order[clamp(i, 0, 3)], 0))

    return pl.pallas_call(
        ffn_kernel,
        grid_spec=pltpu.PrefetchScalarGridSpec(
            num_scalar_prefetch=1,
            grid=(8,),
            in_specs=[whole(), whole(), whole(), whole(), weight_in(), weight_in()]
            + [
                pl.BlockSpec(
                    (1, units, cols), lambda i, order: (0, 0, order[4 + clamp(i - 4, 0, 3)])
                )
            ],
            out_specs=[
                pl.BlockSpec((rows, cols), lambda i, order: (0, clamp(i - 6, 0, 1))),
                pl.BlockSpec((rows, cols), lambda i, order: (0, clamp(i - 4, 0, 1))),
            ],
            scratch_shapes=[
                pltpu.VMEM((rows, units), F32),
                pltpu.VMEM((rows, units), F32),
                pltpu.VMEM((rows, units), BF16),
            ],
        ),
        out_shape=[jax.ShapeDtypeStruct((rows, 2 * cols), BF16)] * 2,
        compiler_params=pltpu.CompilerParams(
            dimension_semantics=("arbitrary",), vmem_limit_bytes=40 * 1024 * 1024
        ),
        cost_estimate=pl.CostEstimate(
            flops=6 * rows * width * units,
            bytes_accessed=6 * width * units + 8 * rows * width,
            transcendentals=rows * units,
        ),
        name="ffn",
    )(order, *pieces, gate_weight, up_weight, down_weight)


def combine_weights(ids_across, weight_across, capacity):
    experts = lax.axis_size("ep")
    rows = ids_across.shape[1]
    numbers = jnp.arange(experts, dtype=jnp.int32)[:, None]
    first = ids_across[0:1] == numbers
    second = ids_across[1:2] == numbers
    named = first | second
    before = jnp.triu(jnp.ones((rows, rows), BF16), 1)
    rank = jnp.dot(named.astype(BF16), before, preferred_element_type=F32)
    weight = jnp.where(first, weight_across[0:1], 0.0) + jnp.where(second, weight_across[1:2], 0.0)
    slot = jnp.arange(capacity, dtype=jnp.int32).astype(F32)[None, :, None]
    held = (rank[:, None, :] == slot) & named[:, None, :]
    return jnp.where(held, weight[:, None, :], 0.0).reshape(experts * capacity, rows)


def shards(
    queries,
    key_rows,
    value_rows,
    head_lambda,
    sub_gain,
    out_weight,
    expert_input,
    norm_gain,
    route_ids,
    route_weight,
    gate_weight,
    up_weight,
    down_weight,
):
    rows_b, width = expert_input.shape
    experts = lax.axis_size("ep")
    capacity = 5 * route_ids.shape[1] * rows_b // (3 * experts)
    slots = experts * capacity
    place = lax.axis_index("tp").astype(jnp.int32)
    cols = width // lax.axis_size("tp")
    ids_across = route_ids.T
    weight_across = route_weight.T

    outgoing = dispatched(expert_input, norm_gain, ids_across, capacity)
    own = lax.all_to_all(
        outgoing.reshape(experts, capacity, cols), "ep", split_axis=0, concat_axis=0, tiled=True
    ).reshape(slots, cols)
    far = swap(own, "tp", 2)
    near = swap(own, "tp", 1)
    near_far = swap(far, "tp", 1)

    key_in, value_in, own_done = lax.optimization_barrier((key_rows, value_rows, own))
    both, places = gathered_keys(key_in, value_in)
    share = attention(queries, both, places, head_lambda, sub_gain, out_weight)
    parts = lax.all_to_all(
        share.reshape(lax.axis_size("tp"), -1, share.shape[1]), "tp", 0, 0, tiled=True
    )
    mixer_out = jnp.sum(parts.astype(F32), axis=0).astype(BF16)

    order = jnp.array([0, 1, 2, 3, 1, 3, 0, 2], jnp.int32) ^ place
    keep, send = ffn(order, (own, near, far, near_far), gate_weight, up_weight, down_weight)
    got = swap(send, "tp", 1)
    across = (keep[:, cols:].astype(F32) + got[:, cols:].astype(F32)).astype(BF16)
    got_across = swap(across, "tp", 2)
    mine = keep[:, :cols].astype(F32) + got[:, :cols].astype(F32)
    summed = (mine + got_across.astype(F32)).astype(BF16)
    returned = lax.all_to_all(
        summed.reshape(experts, capacity, cols), "ep", split_axis=0, concat_axis=0, tiled=True
    ).reshape(slots, cols)
    mixed = lax.dot_general(
        combine_weights(ids_across, weight_across, capacity),
        returned.astype(F32),
        (((0,), (0,)), ((), ())),
        precision=lax.Precision.HIGHEST,
        preferred_element_type=F32,
    )
    return (mixer_out, mixed.astype(BF16))


def solution(mesh):
    placed = (
        P("ep", "tp"),
        P("ep", "tp"),
        P("ep", "tp"),
        P("tp"),
        P(),
        P("tp", None),
        P("ep", None),
        P(),
        P("ep", None),
        P("ep", None),
        P("ep", None, "tp"),
        P("ep", None, "tp"),
        P("ep", "tp", None),
    )
    return jax.shard_map(
        shards,
        mesh=mesh,
        in_specs=placed,
        out_specs=(P(("ep", "tp"), None), P("ep", "tp")),
        check_vma=False,
    )
```

```python
import functools

import jax
import jax.numpy as jnp
from jax import lax
from jax.experimental import pallas as pl
from jax.experimental.pallas import tpu as pltpu
from jax.sharding import PartitionSpec as P

EPS = 1e-06
F32 = jnp.float32
BF16 = jnp.bfloat16


def swap(x, axis, mask):
    count = lax.axis_size(axis)
    return lax.ppermute(x, axis, [(i, i ^ mask) for i in range(count)])


def later(x, axis, step):
    count = lax.axis_size(axis)
    return lax.ppermute(x, axis, [(i, i + step) for i in range(count - step)])


def gathered_keys(key_rows, value_rows):
    count = lax.axis_size("ep")
    own = jnp.concatenate([key_rows, value_rows], axis=1)
    both = lax.all_gather(own, "ep", axis=0, tiled=True)
    return both, jnp.arange(count, dtype=jnp.int32)


def attention(queries, both, places, head_lambda, sub_gain, out_weight):
    rows_here = queries.shape[0]
    heads_here = head_lambda.shape[0]
    head_width = queries.shape[1] // (2 * heads_here)
    width = queries.shape[1]
    value_width = (both.shape[1] - width) // heads_here
    scaling = head_width ** (-0.5)
    length = both.shape[0]
    query_blocks = queries.reshape(rows_here, heads_here, 2, head_width)
    query_pos = lax.axis_index("ep") * rows_here + jnp.arange(rows_here, dtype=jnp.int32)
    key_pos = (
        places[:, None] * rows_here + jnp.arange(rows_here, dtype=jnp.int32)[None, :]
    ).reshape(length)
    key_blocks = both[:, :width].reshape(length, heads_here, 2, head_width)
    value_blocks = both[:, width:].reshape(length, heads_here, value_width)
    scores = (
        jnp.einsum("qhmd,khmd->hmqk", query_blocks, key_blocks, preferred_element_type=F32)
        * scaling
    )
    allowed = (query_pos[:, None] >= key_pos[None, :]) & (key_pos[None, :] >= 0)
    scores = jnp.where(allowed, scores, -1e30)
    row_max = jnp.max(scores, axis=-1)
    weights = jnp.where(allowed, jnp.exp(scores - row_max[..., None]), 0.0)
    row_total = jnp.sum(weights, axis=-1)
    numerator = jnp.einsum(
        "hmqk,khd->hmqd", weights.astype(BF16), value_blocks, preferred_element_type=F32
    )
    per_map = numerator / row_total[..., None]
    contrast = per_map[:, 0] - head_lambda[:, None, None] * per_map[:, 1]
    normed = (
        contrast * lax.rsqrt(jnp.mean(contrast * contrast, axis=-1, keepdims=True) + EPS) * sub_gain
    ).astype(BF16)
    attended = jnp.transpose(normed, (1, 0, 2)).reshape(rows_here, heads_here * value_width)
    return jnp.dot(attended, out_weight, preferred_element_type=F32).astype(BF16)


VMEM = pl.BlockSpec(memory_space=pltpu.VMEM)
SMEM = pl.BlockSpec(memory_space=pltpu.SMEM)


def half(index, size):
    return pl.ds(pl.multiple_of(index * size, size), size)


def pick_kernel(place_ref, query_ref, key_ref, value_ref, out_ref):
    other = 1 - (place_ref[0] & 1)
    at = 0
    for ref in (query_ref, key_ref, value_ref):
        wide = ref.shape[1] // 2
        out_ref[:, at : at + wide] = ref[:, half(other, wide)]
        at += wide


def merge_kernel(place_ref, query_ref, key_ref, value_ref, got_ref, query_out, block_out):
    mine = place_ref[0] & 1
    rows = query_ref.shape[0]
    pair, deep = key_ref.shape[1] // 2, value_ref.shape[1] // 2
    own, other = half(mine, rows), half(1 - mine, rows)
    query_out[own, :] = query_ref[:, half(mine, pair)]
    query_out[other, :] = got_ref[:, :pair]
    block_out[own, :pair] = key_ref[:, half(mine, pair)]
    block_out[own, pair:] = value_ref[:, half(mine, deep)]
    block_out[other, :] = got_ref[:, pair:]


def attention_kernel(head_width, place_ref, lambda_ref, query_ref, own_ref, *rest):
    lines = rest[:-4]
    gain_ref, keep_ref, send_ref, attended = rest[-4:]
    rows = query_ref.shape[0] // 2
    pair = 2 * head_width
    mine, line_place = place_ref[0] & 1, place_ref[0] >> 1
    causal = lax.broadcasted_iota(jnp.int32, (rows, rows), 0) >= lax.broadcasted_iota(
        jnp.int32, (rows, rows), 1
    )
    lane = lax.broadcasted_iota(jnp.int32, (rows, pair), 1)
    scaling = head_width ** (-0.5)
    lam = lambda_ref[mine]
    for side in range(2):
        query = query_ref[side * rows : (side + 1) * rows, :].astype(F32)
        pieces = [(own_ref, side * rows, rows, None)]
        if side:
            pieces.append((own_ref, 0, rows, 0.0))
        for k, ref in enumerate(lines):
            bias = jnp.where(line_place >= k + 1, 0.0, -1e30).astype(F32)
            pieces += [(ref, 0, rows, bias), (ref, rows, rows, bias)]
        per_map = []
        for m in range(2):
            one = jnp.where(lane // head_width == m, query, 0.0).astype(BF16)
            scores = []
            for ref, first, count, bias in pieces:
                s = scaling * lax.dot_general(
                    one,
                    ref[first : first + count, :pair],
                    (((1,), (1,)), ((), ())),
                    preferred_element_type=F32,
                )
                scores.append(jnp.where(causal, s, -1e30) if bias is None else s + bias)
            top = jnp.max(functools.reduce(jnp.maximum, scores), axis=-1, keepdims=True)
            weights = [jnp.exp(s - top) for s in scores]
            row_sum = jnp.sum(functools.reduce(jnp.add, weights), axis=-1, keepdims=True)
            numerator = functools.reduce(
                jnp.add,
                [
                    jnp.dot(
                        w.astype(BF16),
                        ref[first : first + count, pair:],
                        preferred_element_type=F32,
                    )
                    for w, (ref, first, count, _) in zip(weights, pieces)
                ],
            )
            per_map.append(numerator / row_sum)
        contrast = per_map[0] - lam * per_map[1]
        square = jnp.mean(contrast * contrast, axis=-1, keepdims=True)
        attended[side * rows : (side + 1) * rows, :] = (
            contrast * lax.rsqrt(square + EPS) * gain_ref[...]
        ).astype(BF16)
    keep_ref[...] = attended[half(mine, rows), :]
    send_ref[...] = attended[half(1 - mine, rows), :]


def project_kernel(place_ref, own_ref, got_ref, weight_ref, keep_ref, send_ref, attended):
    mine, place = place_ref[0] & 1, place_ref[1]
    rows, deep = own_ref.shape
    attended[:, half(mine, deep)] = own_ref[...]
    attended[:, half(1 - mine, deep)] = got_ref[...]
    group = rows // 4
    for out_ref, masks in ((send_ref, (1, 3)), (keep_ref, (0, 2))):
        picked = [attended[half(place ^ mask, group), :] for mask in masks]
        out_ref[...] = jnp.dot(
            jnp.concatenate(picked, axis=0), weight_ref[...], preferred_element_type=F32
        ).astype(BF16)


def local(kernel, outs, operands, smem=1, scratch=(), flops=1000000, limit=20):
    size = sum(x.size for x in operands)
    return pl.pallas_call(
        kernel,
        out_shape=[jax.ShapeDtypeStruct(shape, BF16) for shape in outs],
        in_specs=[SMEM] * smem + [VMEM] * (len(operands) - smem),
        out_specs=[VMEM] * len(outs),
        scratch_shapes=list(scratch),
        compiler_params=pltpu.CompilerParams(vmem_limit_bytes=limit * 1024 * 1024),
        cost_estimate=pl.CostEstimate(
            flops=flops, bytes_accessed=2 * size, transcendentals=0
        ),
    )(*operands)


def dispatch_kernel(
    experts, capacity, place_ref, ids_ref, rows_ref, gain_ref, out_ref, onehot_ref
):
    rows, _ = rows_ref.shape
    cols = out_ref.shape[1]
    first = pl.multiple_of(place_ref[0] * cols, cols)
    wide = rows_ref[...].astype(F32)
    scale = lax.rsqrt(jnp.mean(wide * wide, axis=-1, keepdims=True) + EPS)
    part = rows_ref[:, pl.ds(first, cols)].astype(F32)
    normed = (part * scale * gain_ref[:, pl.ds(first, cols)]).astype(BF16)
    numbers = lax.broadcasted_iota(jnp.int32, (experts, rows), 0)
    named = (ids_ref[0:1, :] == numbers) | (ids_ref[1:2, :] == numbers)
    before = (
        lax.broadcasted_iota(jnp.int32, (rows, rows), 0)
        < lax.broadcasted_iota(jnp.int32, (rows, rows), 1)
    ).astype(F32).astype(BF16)
    rank = jnp.dot(named.astype(F32).astype(BF16), before, preferred_element_type=F32)
    rank = jnp.where(named, rank, -1.0)
    slot = lax.broadcasted_iota(jnp.int32, (capacity, rows), 0).astype(F32)
    for e in range(experts):
        onehot_ref[e * capacity : (e + 1) * capacity, :] = (
            rank[e : e + 1, :] == slot
        ).astype(F32)
    out_ref[...] = jnp.dot(
        onehot_ref[...].astype(BF16), normed, preferred_element_type=F32
    ).astype(BF16)


def dispatched(expert_input, norm_gain, ids_across, capacity):
    rows, width = expert_input.shape
    experts = lax.axis_size("ep")
    cols = width // lax.axis_size("tp")
    slots = experts * capacity
    vmem = pl.BlockSpec(memory_space=pltpu.VMEM)
    return pl.pallas_call(
        functools.partial(dispatch_kernel, experts, capacity),
        out_shape=jax.ShapeDtypeStruct((slots, cols), BF16),
        in_specs=[pl.BlockSpec(memory_space=pltpu.SMEM), vmem, vmem, vmem],
        out_specs=vmem,
        scratch_shapes=[pltpu.VMEM((slots, rows), F32)],
        cost_estimate=pl.CostEstimate(
            flops=2 * slots * rows * cols, bytes_accessed=2 * rows * width, transcendentals=rows
        ),
        name="dispatch",
    )(
        lax.axis_index("tp").astype(jnp.int32).reshape(1),
        ids_across,
        expert_input,
        norm_gain.reshape(1, width),
    )


def fetch_kernel(gate, up, down, gate_w, up_w, down_w, sem):
    copies = []
    for n, (source, target) in enumerate(((gate, gate_w), (up, up_w), (down, down_w))):
        part = target.shape[0] // 4
        for k in range(4):
            rows = slice(k * part, (k + 1) * part)
            copies.append(
                pltpu.make_async_copy(source.at[0, rows, :], target.at[rows, :], sem.at[4 * n + k])
            )
    for copy in copies:
        copy.start()
    for copy in copies:
        copy.wait()


def fetched(*weights):
    hbm = pl.BlockSpec(memory_space=pltpu.HBM)
    vmem = pl.BlockSpec(memory_space=pltpu.VMEM)
    return pl.pallas_call(
        fetch_kernel,
        in_specs=[hbm] * 3,
        out_specs=[vmem] * 3,
        out_shape=[pltpu.VMEM(w.shape[1:], w.dtype) for w in weights],
        scratch_shapes=[pltpu.SemaphoreType.DMA((12,))],
        compiler_params=pltpu.CompilerParams(vmem_limit_bytes=24 * 1024 * 1024),
        cost_estimate=pl.CostEstimate(
            flops=sum(w.size for w in weights) * 100,
            bytes_accessed=sum(w.size for w in weights) * 2,
            transcendentals=0,
        ),
        name="fetch",
    )(*(pltpu.with_memory_space_constraint(w, pltpu.HBM) for w in weights))


def ffn_kernel(
    first, order_ref, own, near, far, cross, gate_w, up_w, down_w, keep_ref, send_ref
):
    rows, cols = far.shape
    pieces = (own[first : first + rows, :], near[first : first + rows, :], far[...], cross[...])

    def part(k):
        return pl.ds(pl.multiple_of(order_ref[k] * cols, cols), cols)

    def product(weight_w):
        return functools.reduce(
            jnp.add,
            [
                jnp.dot(piece, weight_w[part(k), :], preferred_element_type=F32)
                for k, piece in enumerate(pieces)
            ],
        )

    gate_act = product(gate_w)
    up_act = product(up_w)
    hidden = (gate_act / (1.0 + jnp.exp(-gate_act)) * up_act).astype(BF16)
    for n, out_ref in enumerate((send_ref, keep_ref)):
        for k in range(2):
            out_ref[:, k * cols : (k + 1) * cols] = jnp.dot(
                hidden, down_w[:, part(4 + 2 * n + k)], preferred_element_type=F32
            ).astype(BF16)


def ffn(order, first, own, near, far, cross, weights):
    rows, cols = far.shape
    width, units = weights[0].shape
    vmem = pl.BlockSpec(memory_space=pltpu.VMEM)
    return pl.pallas_call(
        functools.partial(ffn_kernel, first),
        in_specs=[pl.BlockSpec(memory_space=pltpu.SMEM)] + [vmem] * 7,
        out_specs=[vmem, vmem],
        out_shape=[jax.ShapeDtypeStruct((rows, 2 * cols), BF16)] * 2,
        compiler_params=pltpu.CompilerParams(vmem_limit_bytes=30 * 1024 * 1024),
        cost_estimate=pl.CostEstimate(
            flops=6 * rows * width * units,
            bytes_accessed=6 * width * units + 4 * rows * width,
            transcendentals=rows * units,
        ),
        name="ffn",
    )(
        order,
        own,
        near,
        far,
        cross,
        *(pltpu.with_memory_space_constraint(w, pltpu.VMEM) for w in weights),
    )


def total_kernel(*refs):
    out_ref = refs[-1]
    rows, _ = refs[2].shape
    for i in range((len(refs) - 1) // 3):
        keep_ref, got_ref, over_ref = refs[3 * i : 3 * i + 3]
        out_ref[i * rows : (i + 1) * rows, :] = (
            keep_ref[...].astype(F32)
            + got_ref[...].astype(F32)
            + over_ref[...].astype(F32)
        ).astype(BF16)


def total(mine, gots):
    rows, cols = gots[0].shape
    operands = [x for (keep, got), over in zip(mine, gots) for x in (keep, got, over)]
    first = pl.BlockSpec((rows, cols), lambda i: (0, 0))
    return pl.pallas_call(
        total_kernel,
        out_shape=jax.ShapeDtypeStruct((len(gots) * rows, cols), BF16),
        grid=(1,),
        in_specs=[first] * len(operands),
        out_specs=pl.BlockSpec((len(gots) * rows, cols), lambda i: (0, 0)),
        cost_estimate=pl.CostEstimate(
            flops=4 * rows * cols, bytes_accessed=16 * rows * cols, transcendentals=0
        ),
        name="total",
    )(*operands)


def combine_weights(ids_across, weight_across, capacity):
    experts = lax.axis_size("ep")
    rows = ids_across.shape[1]
    numbers = jnp.arange(experts, dtype=jnp.int32)[:, None]
    first = ids_across[0:1] == numbers
    second = ids_across[1:2] == numbers
    named = first | second
    before = jnp.triu(jnp.ones((rows, rows), BF16), 1)
    rank = jnp.dot(named.astype(BF16), before, preferred_element_type=F32)
    weight = jnp.where(first, weight_across[0:1], 0.0) + jnp.where(second, weight_across[1:2], 0.0)
    slot = jnp.arange(capacity, dtype=jnp.int32).astype(F32)[None, :, None]
    held = (rank[:, None, :] == slot) & named[:, None, :]
    return jnp.where(held, weight[:, None, :], 0.0).reshape(experts * capacity, rows)


def shards(
    queries,
    key_rows,
    value_rows,
    head_lambda,
    sub_gain,
    out_weight,
    expert_input,
    norm_gain,
    route_ids,
    route_weight,
    gate_weight,
    up_weight,
    down_weight,
):
    rows_b, width = expert_input.shape
    experts = lax.axis_size("ep")
    capacity = 5 * route_ids.shape[1] * rows_b // (3 * experts)
    slots = experts * capacity
    place = lax.axis_index("tp").astype(jnp.int32)
    cols = width // lax.axis_size("tp")
    ids_across = route_ids.T
    weight_across = route_weight.T

    weights = fetched(gate_weight, up_weight, down_weight)
    outgoing = dispatched(expert_input, norm_gain, ids_across, capacity)
    own = lax.all_to_all(
        outgoing.reshape(experts, capacity, cols), "ep", split_axis=0, concat_axis=0, tiled=True
    ).reshape(slots, cols)
    small = experts <= 8 and experts % 2 == 0 and head_lambda.shape[0] == 2
    here = jnp.stack([lax.axis_index("ep"), lax.axis_index("tp")]).astype(jnp.int32)
    if small:
        rows_a, deep = queries.shape[0], value_rows.shape[1] // 2
        pair = queries.shape[1] // 2
        trio = (queries, key_rows, value_rows)
        (picked,) = local(pick_kernel, [(rows_a, 2 * pair + deep)], (here, *trio))
        got = swap(picked, "ep", 1)
        query, block = local(
            merge_kernel, [(2 * rows_a, pair), (2 * rows_a, pair + deep)], (here, *trio, got)
        )
        block, _ = lax.optimization_barrier((block, own))
    near = swap(own, "tp", 1)
    halves = 2
    part = slots // halves
    order = jnp.array([0, 1, 2, 3, 1, 3, 0, 2], jnp.int32) ^ place
    fars = [swap(own[i * part : (i + 1) * part], "tp", 2) for i in range(halves)]
    if small:
        blocks = [later(block, "ep", 2 * k) for k in range(1, experts // 2)]
    mine, gots = [], []
    for i in range(halves):
        cross = swap(fars[i], "tp", 1)
        keep, send = ffn(
            order, i * part, own, near, fars[i], cross, weights
        )
        got = swap(send, "tp", 1)
        across = (keep[:, cols:].astype(F32) + got[:, cols:].astype(F32)).astype(BF16)
        gots.append(swap(across, "tp", 2))
        mine.append((keep, got))
    if small:
        kept, sent = local(
            functools.partial(attention_kernel, pair // 2),
            [(rows_a, deep)] * 2,
            (here, head_lambda, query, block, *blocks, sub_gain.reshape(1, -1)),
            smem=2,
            scratch=[pltpu.VMEM((2 * rows_a, deep), BF16)],
            flops=16 * rows_a * rows_a * experts * pair,
            limit=28,
        )
        got = swap(sent, "ep", 1)
        model = out_weight.shape[1]
        kept, sent = local(
            project_kernel,
            [(rows_a // 2, model)] * 2,
            (here, kept, got, out_weight),
            scratch=[pltpu.VMEM((rows_a, 2 * deep), BF16)],
            flops=4 * rows_a * deep * model,
        )
        got = swap(sent, "tp", 1)
        group = got.shape[0] // 2
        across = (kept[group:].astype(F32) + got[group:].astype(F32)).astype(BF16)
        last = swap(across, "tp", 2)
        mixer_out = (
            kept[:group].astype(F32) + got[:group].astype(F32) + last.astype(F32)
        ).astype(BF16)
    else:
        key_rows, value_rows, _ = lax.optimization_barrier((key_rows, value_rows, own))
        both, places = gathered_keys(key_rows, value_rows)
        share = attention(queries, both, places, head_lambda, sub_gain, out_weight)
        parts = lax.all_to_all(
            share.reshape(lax.axis_size("tp"), -1, share.shape[1]), "tp", 0, 0, tiled=True
        )
        mixer_out = jnp.sum(parts.astype(F32), axis=0).astype(BF16)
    summed = total(mine, gots)
    returned = lax.all_to_all(
        summed.reshape(experts, capacity, cols), "ep", split_axis=0, concat_axis=0, tiled=True
    ).reshape(slots, cols)
    mixed = lax.dot_general(
        combine_weights(ids_across, weight_across, capacity),
        returned.astype(F32),
        (((0,), (0,)), ((), ())),
        precision=lax.Precision.HIGHEST,
        preferred_element_type=F32,
    )
    return (mixer_out, mixed.astype(BF16))


def solution(mesh):
    placed = (
        P("ep", "tp"),
        P("ep", "tp"),
        P("ep", "tp"),
        P("tp"),
        P(),
        P("tp", None),
        P("ep", None),
        P(),
        P("ep", None),
        P("ep", None),
        P("ep", None, "tp"),
        P("ep", None, "tp"),
        P("ep", "tp", None),
    )

    return jax.shard_map(
        shards,
        mesh=mesh,
        in_specs=placed,
        out_specs=(P(("ep", "tp"), None), P("ep", "tp")),
        check_vma=False,
    )
```

```python
import functools

import jax
import jax.numpy as jnp
from jax import lax
from jax.experimental import pallas as pl
from jax.experimental.pallas import tpu as pltpu
from jax.sharding import PartitionSpec as P

EPS = 1e-06
F32 = jnp.float32
BF16 = jnp.bfloat16


def swap(x, axis, mask):
    count = lax.axis_size(axis)
    return lax.ppermute(x, axis, [(i, i ^ mask) for i in range(count)])


def ep_of(here_ref):
    return lax.div(here_ref[0], lax.axis_size("tp"))


def tp_of(here_ref):
    return lax.rem(here_ref[0], lax.axis_size("tp"))


def onward(x, axis, step, first):
    count = lax.axis_size(axis)
    return lax.ppermute(x, axis, [(i, i + step) for i in range(first, count - step)])


def gathered_keys(key_rows, value_rows):
    count = lax.axis_size("ep")
    own = jnp.concatenate([key_rows, value_rows], axis=1)
    both = lax.all_gather(own, "ep", axis=0, tiled=True)
    return both, jnp.arange(count, dtype=jnp.int32)


def attention(queries, both, places, head_lambda, sub_gain, out_weight):
    rows_here = queries.shape[0]
    heads_here = head_lambda.shape[0]
    head_width = queries.shape[1] // (2 * heads_here)
    width = queries.shape[1]
    value_width = (both.shape[1] - width) // heads_here
    scaling = head_width ** (-0.5)
    length = both.shape[0]
    query_blocks = queries.reshape(rows_here, heads_here, 2, head_width)
    query_pos = lax.axis_index("ep") * rows_here + jnp.arange(rows_here, dtype=jnp.int32)
    key_pos = (
        places[:, None] * rows_here + jnp.arange(rows_here, dtype=jnp.int32)[None, :]
    ).reshape(length)
    key_blocks = both[:, :width].reshape(length, heads_here, 2, head_width)
    value_blocks = both[:, width:].reshape(length, heads_here, value_width)
    scores = (
        jnp.einsum("qhmd,khmd->hmqk", query_blocks, key_blocks, preferred_element_type=F32)
        * scaling
    )
    allowed = (query_pos[:, None] >= key_pos[None, :]) & (key_pos[None, :] >= 0)
    scores = jnp.where(allowed, scores, -1e30)
    row_max = jnp.max(scores, axis=-1)
    weights = jnp.where(allowed, jnp.exp(scores - row_max[..., None]), 0.0)
    row_total = jnp.sum(weights, axis=-1)
    numerator = jnp.einsum(
        "hmqk,khd->hmqd", weights.astype(BF16), value_blocks, preferred_element_type=F32
    )
    per_map = numerator / row_total[..., None]
    contrast = per_map[:, 0] - head_lambda[:, None, None] * per_map[:, 1]
    normed = (
        contrast * lax.rsqrt(jnp.mean(contrast * contrast, axis=-1, keepdims=True) + EPS) * sub_gain
    ).astype(BF16)
    attended = jnp.transpose(normed, (1, 0, 2)).reshape(rows_here, heads_here * value_width)
    return jnp.dot(attended, out_weight, preferred_element_type=F32).astype(BF16)


VMEM = pl.BlockSpec(memory_space=pltpu.VMEM)
SMEM = pl.BlockSpec(memory_space=pltpu.SMEM)


def half(index, size):
    return pl.ds(pl.multiple_of(index * size, size), size)


def pick_kernel(place_ref, query_ref, key_ref, value_ref, out_ref):
    other = 1 - (ep_of(place_ref) & 1)
    at = 0
    for ref in (query_ref, key_ref, value_ref):
        wide = ref.shape[1] // 2
        out_ref[:, at : at + wide] = ref[:, half(other, wide)]
        at += wide


def merge_kernel(place_ref, query_ref, key_ref, value_ref, got_ref, query_out, block_out):
    mine = ep_of(place_ref) & 1
    rows = query_ref.shape[0]
    pair, deep = key_ref.shape[1] // 2, value_ref.shape[1] // 2
    own, other = half(mine, rows), half(1 - mine, rows)
    query_out[own, :] = query_ref[:, half(mine, pair)]
    query_out[other, :] = got_ref[:, :pair]
    block_out[own, :pair] = key_ref[:, half(mine, pair)]
    block_out[own, pair:] = value_ref[:, half(mine, deep)]
    block_out[other, :] = got_ref[:, pair:]


def attention_kernel(head_width, place_ref, lambda_ref, query_ref, own_ref, *rest):
    lines = rest[:-4]
    gain_ref, keep_ref, send_ref, attended = rest[-4:]
    rows = query_ref.shape[0] // 2
    pair = 2 * head_width
    mine, line_place = ep_of(place_ref) & 1, ep_of(place_ref) >> 1
    causal = lax.broadcasted_iota(jnp.int32, (rows, rows), 0) >= lax.broadcasted_iota(
        jnp.int32, (rows, rows), 1
    )
    lane = lax.broadcasted_iota(jnp.int32, (rows, pair), 1)
    scaling = head_width ** (-0.5)
    lam = lambda_ref[mine]
    for side in range(2):
        query = query_ref[side * rows : (side + 1) * rows, :].astype(F32)
        pieces = [(own_ref, side * rows, rows, None)]
        if side:
            pieces.append((own_ref, 0, rows, 0.0))
        for k, ref in enumerate(lines):
            bias = jnp.where(line_place >= k + 1, 0.0, -1e30).astype(F32)
            pieces += [(ref, 0, rows, bias), (ref, rows, rows, bias)]
        per_map = []
        for m in range(2):
            one = jnp.where(lane // head_width == m, query, 0.0).astype(BF16)
            scores = []
            for ref, first, count, bias in pieces:
                s = scaling * lax.dot_general(
                    one,
                    ref[first : first + count, :pair],
                    (((1,), (1,)), ((), ())),
                    preferred_element_type=F32,
                )
                scores.append(jnp.where(causal, s, -1e30) if bias is None else s + bias)
            top = jnp.max(functools.reduce(jnp.maximum, scores), axis=-1, keepdims=True)
            weights = [jnp.exp(s - top) for s in scores]
            row_sum = jnp.sum(functools.reduce(jnp.add, weights), axis=-1, keepdims=True)
            numerator = functools.reduce(
                jnp.add,
                [
                    jnp.dot(
                        w.astype(BF16),
                        ref[first : first + count, pair:],
                        preferred_element_type=F32,
                    )
                    for w, (ref, first, count, _) in zip(weights, pieces)
                ],
            )
            per_map.append(numerator / row_sum)
        contrast = per_map[0] - lam * per_map[1]
        square = jnp.mean(contrast * contrast, axis=-1, keepdims=True)
        attended[side * rows : (side + 1) * rows, :] = (
            contrast * lax.rsqrt(square + EPS) * gain_ref[...]
        ).astype(BF16)
    keep_ref[...] = attended[half(mine, rows), :]
    send_ref[...] = attended[half(1 - mine, rows), :]


def project_kernel(place_ref, own_ref, got_ref, weight_ref, keep_ref, send_ref, attended):
    mine, place = ep_of(place_ref) & 1, tp_of(place_ref)
    rows, deep = own_ref.shape
    attended[:, half(mine, deep)] = own_ref[...]
    attended[:, half(1 - mine, deep)] = got_ref[...]
    group = rows // 4
    for out_ref, masks in ((send_ref, (1, 3)), (keep_ref, (0, 2))):
        picked = [attended[half(place ^ mask, group), :] for mask in masks]
        out_ref[...] = jnp.dot(
            jnp.concatenate(picked, axis=0), weight_ref[...], preferred_element_type=F32
        ).astype(BF16)


def local(kernel, outs, operands, smem=1, scratch=(), flops=1000000, limit=12, far=0):
    size = sum(x.size for x in operands)
    operands = list(operands)
    specs, options = [VMEM] * (len(operands) - smem), {}
    outs_specs = [VMEM] * len(outs)
    if far:
        for n in range(smem, smem + far):
            operands[n] = pltpu.with_memory_space_constraint(operands[n], pltpu.HBM)
        whole = lambda i: (0, 0)
        options["grid"] = (1,)
        specs = [pl.BlockSpec(x.shape, whole) for x in operands[smem:]]
        outs_specs = [pl.BlockSpec(shape, whole) for shape in outs]
    return pl.pallas_call(
        kernel,
        out_shape=[jax.ShapeDtypeStruct(shape, BF16) for shape in outs],
        in_specs=[SMEM] * smem + specs,
        out_specs=outs_specs,
        **options,
        scratch_shapes=list(scratch),
        compiler_params=pltpu.CompilerParams(vmem_limit_bytes=limit * 1024 * 1024),
        cost_estimate=pl.CostEstimate(
            flops=flops, bytes_accessed=2 * size, transcendentals=0
        ),
    )(*operands)


def dispatch_kernel(experts, capacity, here_ref, ids_ref, rows_ref, gain_ref, *rest):
    outs, onehot_ref, rank_ref = rest[:-2], rest[-2], rest[-1]
    rows, _ = rows_ref.shape
    cols = outs[0].shape[1]
    first = pl.multiple_of(tp_of(here_ref) * cols, cols)
    wide = rows_ref[...].astype(F32)
    scale = lax.rsqrt(jnp.mean(wide * wide, axis=-1, keepdims=True) + EPS)
    part = rows_ref[:, pl.ds(first, cols)].astype(F32)
    normed = (part * scale * gain_ref[:, pl.ds(first, cols)]).astype(BF16)
    numbers = lax.broadcasted_iota(jnp.int32, (experts, rows), 0)
    named = (ids_ref[0:1, :] == numbers) | (ids_ref[1:2, :] == numbers)
    before = (
        lax.broadcasted_iota(jnp.int32, (rows, rows), 0)
        < lax.broadcasted_iota(jnp.int32, (rows, rows), 1)
    ).astype(F32).astype(BF16)
    rank = jnp.dot(named.astype(F32).astype(BF16), before, preferred_element_type=F32)
    rank_ref[...] = jnp.where(named, rank, -1.0)
    slot = lax.broadcasted_iota(jnp.int32, (capacity, rows), 0).astype(F32)
    for k in range(experts):
        e = ep_of(here_ref) ^ k if len(outs) > 1 else k
        onehot_ref[k * capacity : (k + 1) * capacity, :] = (
            rank_ref[pl.ds(e, 1), :] == slot
        ).astype(F32)
    count = onehot_ref.shape[0] // len(outs)
    for k, out_ref in enumerate(outs):
        out_ref[...] = jnp.dot(
            onehot_ref[k * count : (k + 1) * count, :].astype(BF16),
            normed,
            preferred_element_type=F32,
        ).astype(BF16)


def dispatched(here, expert_input, norm_gain, ids_across, capacity, pieces):
    rows, width = expert_input.shape
    experts = lax.axis_size("ep")
    cols = width // lax.axis_size("tp")
    slots = experts * capacity
    return pl.pallas_call(
        functools.partial(dispatch_kernel, experts, capacity),
        out_shape=[jax.ShapeDtypeStruct((slots // pieces, cols), BF16)] * pieces,
        in_specs=[SMEM, VMEM, VMEM, VMEM],
        out_specs=[VMEM] * pieces,
        scratch_shapes=[pltpu.VMEM((slots, rows), F32), pltpu.VMEM((experts, rows), F32)],
        cost_estimate=pl.CostEstimate(
            flops=2 * slots * rows * cols, bytes_accessed=2 * rows * width, transcendentals=rows
        ),
        name="dispatch",
    )(here, ids_across, expert_input, norm_gain.reshape(1, width))


def arrange_kernel(here_ref, *refs):
    out_ref = refs[-1]
    for k, ref in enumerate(refs[:-1]):
        out_ref[half(ep_of(here_ref) ^ k, ref.shape[0]), :] = ref[...]


def fetch_kernel(gate, up, down, gate_w, up_w, down_w, sem):
    copies = []
    for n, (source, target) in enumerate(((gate, gate_w), (up, up_w), (down, down_w))):
        part = target.shape[0] // 4
        for k in range(4):
            rows = slice(k * part, (k + 1) * part)
            copies.append(
                pltpu.make_async_copy(source.at[0, rows, :], target.at[rows, :], sem.at[4 * n + k])
            )
    for copy in copies:
        copy.start()
    for copy in copies:
        copy.wait()


def fetched(*weights):
    hbm = pl.BlockSpec(memory_space=pltpu.HBM)
    vmem = pl.BlockSpec(memory_space=pltpu.VMEM)
    return pl.pallas_call(
        fetch_kernel,
        in_specs=[hbm] * 3,
        out_specs=[vmem] * 3,
        out_shape=[pltpu.VMEM(w.shape[1:], w.dtype) for w in weights],
        scratch_shapes=[pltpu.SemaphoreType.DMA((12,))],
        compiler_params=pltpu.CompilerParams(vmem_limit_bytes=4 * 1024 * 1024),
        cost_estimate=pl.CostEstimate(
            flops=sum(w.size for w in weights) * 100,
            bytes_accessed=sum(w.size for w in weights) * 2,
            transcendentals=0,
        ),
        name="fetch",
    )(*(pltpu.with_memory_space_constraint(w, pltpu.HBM) for w in weights))


def ffn_kernel(
    first, order_ref, own, near, far, cross, gate_w, up_w, down_w, keep_ref, send_ref
):
    rows, cols = far.shape
    pieces = (own[first : first + rows, :], near[first : first + rows, :], far[...], cross[...])

    def part(k):
        return pl.ds(pl.multiple_of(order_ref[k] * cols, cols), cols)

    def product(weight_w):
        return functools.reduce(
            jnp.add,
            [
                jnp.dot(piece, weight_w[part(k), :], preferred_element_type=F32)
                for k, piece in enumerate(pieces)
            ],
        )

    gate_act = product(gate_w)
    up_act = product(up_w)
    hidden = (gate_act / (1.0 + jnp.exp(-gate_act)) * up_act).astype(BF16)
    for n, out_ref in enumerate((send_ref, keep_ref)):
        for k in range(2):
            out_ref[:, k * cols : (k + 1) * cols] = jnp.dot(
                hidden, down_w[:, part(4 + 2 * n + k)], preferred_element_type=F32
            ).astype(BF16)


def ffn(order, first, own, near, far, cross, weights):
    rows, cols = far.shape
    width, units = weights[0].shape
    vmem = pl.BlockSpec(memory_space=pltpu.VMEM)
    return pl.pallas_call(
        functools.partial(ffn_kernel, first),
        in_specs=[pl.BlockSpec(memory_space=pltpu.SMEM)] + [vmem] * 7,
        out_specs=[vmem, vmem],
        out_shape=[jax.ShapeDtypeStruct((rows, 2 * cols), BF16)] * 2,
        compiler_params=pltpu.CompilerParams(vmem_limit_bytes=16 * 1024 * 1024),
        cost_estimate=pl.CostEstimate(
            flops=6 * rows * width * units,
            bytes_accessed=6 * width * units + 4 * rows * width,
            transcendentals=rows * units,
        ),
        name="ffn",
    )(
        order,
        own,
        near,
        far,
        cross,
        *(pltpu.with_memory_space_constraint(w, pltpu.VMEM) for w in weights),
    )


def total_kernel(first, keep_ref, got_ref, over_ref, *rest):
    out_ref, part, sem = rest[-3:]
    rows, cols = part.shape
    part[...] = (
        keep_ref[:, :cols].astype(F32) + got_ref[:, :cols].astype(F32) + over_ref[...].astype(F32)
    ).astype(BF16)
    copy = pltpu.make_async_copy(part, out_ref.at[first : first + rows, :], sem)
    copy.start()
    copy.wait()


def total(slots, first, keep, got, over, held=None):
    rows, cols = over.shape
    hbm = pl.BlockSpec(memory_space=pltpu.HBM)
    operands = [keep, got, over] + ([] if held is None else [held])
    return pl.pallas_call(
        functools.partial(total_kernel, first),
        out_shape=jax.ShapeDtypeStruct((slots, cols), BF16),
        in_specs=[VMEM] * 3 + [hbm] * (len(operands) - 3),
        out_specs=hbm,
        scratch_shapes=[pltpu.VMEM((rows, cols), BF16), pltpu.SemaphoreType.DMA],
        input_output_aliases={} if held is None else {3: 0},
        compiler_params=pltpu.CompilerParams(vmem_limit_bytes=8 * 1024 * 1024),
        cost_estimate=pl.CostEstimate(
            flops=4 * rows * cols, bytes_accessed=16 * rows * cols, transcendentals=0
        ),
        name="total",
    )(*operands)


def combine_weights(ids_across, weight_across, capacity):
    experts = lax.axis_size("ep")
    rows = ids_across.shape[1]
    numbers = jnp.arange(experts, dtype=jnp.int32)[:, None]
    first = ids_across[0:1] == numbers
    second = ids_across[1:2] == numbers
    named = first | second
    before = jnp.triu(jnp.ones((rows, rows), BF16), 1)
    rank = jnp.dot(named.astype(BF16), before, preferred_element_type=F32)
    weight = jnp.where(first, weight_across[0:1], 0.0) + jnp.where(second, weight_across[1:2], 0.0)
    slot = jnp.arange(capacity, dtype=jnp.int32).astype(F32)[None, :, None]
    held = (rank[:, None, :] == slot) & named[:, None, :]
    return jnp.where(held, weight[:, None, :], 0.0).reshape(experts * capacity, rows)


def shards(
    queries,
    key_rows,
    value_rows,
    head_lambda,
    sub_gain,
    out_weight,
    expert_input,
    norm_gain,
    route_ids,
    route_weight,
    gate_weight,
    up_weight,
    down_weight,
):
    rows_b, width = expert_input.shape
    experts = lax.axis_size("ep")
    capacity = 5 * route_ids.shape[1] * rows_b // (3 * experts)
    slots = experts * capacity
    place = lax.axis_index("tp").astype(jnp.int32)
    cols = width // lax.axis_size("tp")
    ids_across = route_ids.T
    weight_across = route_weight.T

    weights = fetched(gate_weight, up_weight, down_weight)
    small = experts <= 8 and experts & (experts - 1) == 0 and head_lambda.shape[0] == 2
    here = lax.axis_index("ep") * lax.axis_size("tp") + lax.axis_index("tp")
    here = here.astype(jnp.int32).reshape(1)
    outgoing = dispatched(
        here, expert_input, norm_gain, ids_across, capacity, experts if small else 1
    )
    if small:
        arrived = [outgoing[0]] + [swap(outgoing[k], "ep", k) for k in range(1, experts)]
        (own,) = local(arrange_kernel, [(slots, cols)], (here, *arrived))
    else:
        own = lax.all_to_all(
            outgoing[0].reshape(experts, capacity, cols), "ep", 0, 0, tiled=True
        ).reshape(slots, cols)
    if small:
        rows_a, deep = queries.shape[0], value_rows.shape[1] // 2
        pair = queries.shape[1] // 2
        trio = (queries, key_rows, value_rows)
        (picked,) = local(pick_kernel, [(rows_a, 2 * pair + deep)], (here, *trio), far=3)
        got = swap(picked, "ep", 1)
        query, block = local(
            merge_kernel, [(2 * rows_a, pair), (2 * rows_a, pair + deep)], (here, *trio, got), far=3
        )
    near = swap(own, "tp", 1)
    halves = 2
    part = slots // halves
    order = jnp.array([0, 1, 2, 3, 1, 3, 0, 2], jnp.int32) ^ place
    fars = [swap(own[i * part : (i + 1) * part], "tp", 2) for i in range(halves)]
    if small:
        blocks = []
        for k in range(1, experts // 2):
            moving = blocks[k - 3] if k > 2 else block
            blocks.append(onward(moving, "ep", 2 * min(k, 2), 2 * max(k - 2, 0)))
    mine, gots = [], []
    for i in range(halves):
        cross = swap(fars[i], "tp", 1)
        keep, send = ffn(order, i * part, own, near, fars[i], cross, weights)
        got = swap(send, "tp", 1)
        across = (keep[:, cols:].astype(F32) + got[:, cols:].astype(F32)).astype(BF16)
        gots.append(swap(across, "tp", 2))
        mine.append((keep, got))
    if small:
        kept, sent = local(
            functools.partial(attention_kernel, pair // 2),
            [(rows_a, deep)] * 2,
            (here, head_lambda, query, block, *blocks, sub_gain.reshape(1, -1)),
            smem=2,
            scratch=[pltpu.VMEM((2 * rows_a, deep), BF16)],
            flops=16 * rows_a * rows_a * experts * pair,
            limit=20,
        )
        got = swap(sent, "ep", 1)
        model = out_weight.shape[1]
        kept, sent = local(
            project_kernel,
            [(rows_a // 2, model)] * 2,
            (here, kept, got, out_weight),
            scratch=[pltpu.VMEM((rows_a, 2 * deep), BF16)],
            flops=4 * rows_a * deep * model,
        )
        got = swap(sent, "tp", 1)
        group = got.shape[0] // 2
        across = (kept[group:].astype(F32) + got[group:].astype(F32)).astype(BF16)
        last = swap(across, "tp", 2)
        mixer_out = (
            kept[:group].astype(F32) + got[:group].astype(F32) + last.astype(F32)
        ).astype(BF16)
    else:
        key_rows, value_rows, _ = lax.optimization_barrier((key_rows, value_rows, own))
        both, places = gathered_keys(key_rows, value_rows)
        share = attention(queries, both, places, head_lambda, sub_gain, out_weight)
        parts = lax.all_to_all(
            share.reshape(lax.axis_size("tp"), -1, share.shape[1]), "tp", 0, 0, tiled=True
        )
        mixer_out = jnp.sum(parts.astype(F32), axis=0).astype(BF16)
    summed = None
    for i, ((keep, got), over) in enumerate(zip(mine, gots)):
        summed = total(slots, i * part, keep, got, over, summed)
    returned = lax.all_to_all(
        summed.reshape(experts, capacity, cols), "ep", split_axis=0, concat_axis=0, tiled=True
    ).reshape(slots, cols)
    mixed = lax.dot_general(
        combine_weights(ids_across, weight_across, capacity),
        returned.astype(F32),
        (((0,), (0,)), ((), ())),
        precision=lax.Precision.HIGHEST,
        preferred_element_type=F32,
    )
    return (mixer_out, mixed.astype(BF16))


def solution(mesh):
    placed = (
        P("ep", "tp"),
        P("ep", "tp"),
        P("ep", "tp"),
        P("tp"),
        P(),
        P("tp", None),
        P("ep", None),
        P(),
        P("ep", None),
        P("ep", None),
        P("ep", None, "tp"),
        P("ep", None, "tp"),
        P("ep", "tp", None),
    )

    return jax.shard_map(
        shards,
        mesh=mesh,
        in_specs=placed,
        out_specs=(P(("ep", "tp"), None), P("ep", "tp")),
        check_vma=False,
    )
```

```python
import functools

import jax
import jax.numpy as jnp
from jax import lax
from jax.experimental import pallas as pl
from jax.experimental.pallas import tpu as pltpu
from jax.sharding import PartitionSpec as P

EPS = 1e-06
F32 = jnp.float32
BF16 = jnp.bfloat16


def swap(x, axis, mask):
    count = lax.axis_size(axis)
    return lax.ppermute(x, axis, [(i, i ^ mask) for i in range(count)])


def ep_of(here_ref):
    return lax.div(here_ref[0], lax.axis_size("tp"))


def tp_of(here_ref):
    return lax.rem(here_ref[0], lax.axis_size("tp"))


def onward(x, axis, step, first):
    count = lax.axis_size(axis)
    return lax.ppermute(x, axis, [(i, i + step) for i in range(first, count - step)])


def gathered_keys(key_rows, value_rows):
    count = lax.axis_size("ep")
    own = jnp.concatenate([key_rows, value_rows], axis=1)
    both = lax.all_gather(own, "ep", axis=0, tiled=True)
    return both, jnp.arange(count, dtype=jnp.int32)


def attention(queries, both, places, head_lambda, sub_gain, out_weight):
    rows_here = queries.shape[0]
    heads_here = head_lambda.shape[0]
    head_width = queries.shape[1] // (2 * heads_here)
    width = queries.shape[1]
    value_width = (both.shape[1] - width) // heads_here
    scaling = head_width ** (-0.5)
    length = both.shape[0]
    query_blocks = queries.reshape(rows_here, heads_here, 2, head_width)
    query_pos = lax.axis_index("ep") * rows_here + jnp.arange(rows_here, dtype=jnp.int32)
    key_pos = (
        places[:, None] * rows_here + jnp.arange(rows_here, dtype=jnp.int32)[None, :]
    ).reshape(length)
    key_blocks = both[:, :width].reshape(length, heads_here, 2, head_width)
    value_blocks = both[:, width:].reshape(length, heads_here, value_width)
    scores = (
        jnp.einsum("qhmd,khmd->hmqk", query_blocks, key_blocks, preferred_element_type=F32)
        * scaling
    )
    allowed = (query_pos[:, None] >= key_pos[None, :]) & (key_pos[None, :] >= 0)
    scores = jnp.where(allowed, scores, -1e30)
    row_max = jnp.max(scores, axis=-1)
    weights = jnp.where(allowed, jnp.exp(scores - row_max[..., None]), 0.0)
    row_total = jnp.sum(weights, axis=-1)
    numerator = jnp.einsum(
        "hmqk,khd->hmqd", weights.astype(BF16), value_blocks, preferred_element_type=F32
    )
    per_map = numerator / row_total[..., None]
    contrast = per_map[:, 0] - head_lambda[:, None, None] * per_map[:, 1]
    normed = (
        contrast * lax.rsqrt(jnp.mean(contrast * contrast, axis=-1, keepdims=True) + EPS) * sub_gain
    ).astype(BF16)
    attended = jnp.transpose(normed, (1, 0, 2)).reshape(rows_here, heads_here * value_width)
    return jnp.dot(attended, out_weight, preferred_element_type=F32).astype(BF16)


VMEM = pl.BlockSpec(memory_space=pltpu.VMEM)
SMEM = pl.BlockSpec(memory_space=pltpu.SMEM)


def half(index, size):
    return pl.ds(pl.multiple_of(index * size, size), size)


def pick_kernel(place_ref, query_ref, key_ref, value_ref, out_ref):
    other = 1 - (ep_of(place_ref) & 1)
    at = 0
    for ref in (query_ref, key_ref, value_ref):
        wide = ref.shape[1] // 2
        out_ref[:, at : at + wide] = ref[:, half(other, wide)]
        at += wide


def merge_kernel(place_ref, query_ref, key_ref, value_ref, got_ref, query_out, block_out):
    mine = ep_of(place_ref) & 1
    rows = query_ref.shape[0]
    pair, deep = key_ref.shape[1] // 2, value_ref.shape[1] // 2
    own, other = half(mine, rows), half(1 - mine, rows)
    query_out[own, :] = query_ref[:, half(mine, pair)]
    query_out[other, :] = got_ref[:, :pair]
    block_out[own, :pair] = key_ref[:, half(mine, pair)]
    block_out[own, pair:] = value_ref[:, half(mine, deep)]
    block_out[other, :] = got_ref[:, pair:]


def attention_kernel(head_width, place_ref, lambda_ref, query_ref, own_ref, *rest):
    lines = rest[:-4]
    gain_ref, keep_ref, send_ref, attended = rest[-4:]
    rows = query_ref.shape[0] // 2
    pair = 2 * head_width
    mine, line_place = ep_of(place_ref) & 1, ep_of(place_ref) >> 1
    causal = lax.broadcasted_iota(jnp.int32, (rows, rows), 0) >= lax.broadcasted_iota(
        jnp.int32, (rows, rows), 1
    )
    lane = lax.broadcasted_iota(jnp.int32, (rows, pair), 1)
    scaling = head_width ** (-0.5)
    lam = lambda_ref[mine]
    for side in range(2):
        query = query_ref[side * rows : (side + 1) * rows, :].astype(F32)
        pieces = [(own_ref, side * rows, rows, None)]
        if side:
            pieces.append((own_ref, 0, rows, 0.0))
        for k, ref in enumerate(lines):
            bias = jnp.where(line_place >= k + 1, 0.0, -1e30).astype(F32)
            pieces += [(ref, 0, rows, bias), (ref, rows, rows, bias)]
        per_map = []
        for m in range(2):
            one = jnp.where(lane // head_width == m, query, 0.0).astype(BF16)
            scores = []
            for ref, first, count, bias in pieces:
                s = scaling * lax.dot_general(
                    one,
                    ref[first : first + count, :pair],
                    (((1,), (1,)), ((), ())),
                    preferred_element_type=F32,
                )
                scores.append(jnp.where(causal, s, -1e30) if bias is None else s + bias)
            top = jnp.max(functools.reduce(jnp.maximum, scores), axis=-1, keepdims=True)
            weights = [jnp.exp(s - top) for s in scores]
            row_sum = jnp.sum(functools.reduce(jnp.add, weights), axis=-1, keepdims=True)
            numerator = functools.reduce(
                jnp.add,
                [
                    jnp.dot(
                        w.astype(BF16),
                        ref[first : first + count, pair:],
                        preferred_element_type=F32,
                    )
                    for w, (ref, first, count, _) in zip(weights, pieces)
                ],
            )
            per_map.append(numerator / row_sum)
        contrast = per_map[0] - lam * per_map[1]
        square = jnp.mean(contrast * contrast, axis=-1, keepdims=True)
        attended[side * rows : (side + 1) * rows, :] = (
            contrast * lax.rsqrt(square + EPS) * gain_ref[...]
        ).astype(BF16)
    keep_ref[...] = attended[half(mine, rows), :]
    send_ref[...] = attended[half(1 - mine, rows), :]


def project_kernel(place_ref, own_ref, got_ref, weight_ref, keep_ref, send_ref, attended):
    mine, place = ep_of(place_ref) & 1, tp_of(place_ref)
    rows, deep = own_ref.shape
    attended[:, half(mine, deep)] = own_ref[...]
    attended[:, half(1 - mine, deep)] = got_ref[...]
    group = rows // 4
    for out_ref, masks in ((send_ref, (1, 3)), (keep_ref, (0, 2))):
        picked = [attended[half(place ^ mask, group), :] for mask in masks]
        out_ref[...] = jnp.dot(
            jnp.concatenate(picked, axis=0), weight_ref[...], preferred_element_type=F32
        ).astype(BF16)


def local(kernel, outs, operands, smem=1, scratch=(), flops=1000000, limit=12, far=0):
    size = sum(x.size for x in operands)
    operands = list(operands)
    specs, options = [VMEM] * (len(operands) - smem), {}
    outs_specs = [VMEM] * len(outs)
    if far:
        for n in range(smem, smem + far):
            operands[n] = pltpu.with_memory_space_constraint(operands[n], pltpu.HBM)
        whole = lambda i: (0, 0)
        options["grid"] = (1,)
        specs = [pl.BlockSpec(x.shape, whole) for x in operands[smem:]]
        outs_specs = [pl.BlockSpec(shape, whole) for shape in outs]
    return pl.pallas_call(
        kernel,
        out_shape=[jax.ShapeDtypeStruct(shape, BF16) for shape in outs],
        in_specs=[SMEM] * smem + specs,
        out_specs=outs_specs,
        **options,
        scratch_shapes=list(scratch),
        compiler_params=pltpu.CompilerParams(vmem_limit_bytes=limit * 1024 * 1024),
        cost_estimate=pl.CostEstimate(
            flops=flops, bytes_accessed=2 * size, transcendentals=0
        ),
    )(*operands)


def dispatch_kernel(experts, capacity, here_ref, ids_ref, rows_ref, gain_ref, *rest):
    outs, onehot_ref, rank_ref = rest[:-2], rest[-2], rest[-1]
    rows, _ = rows_ref.shape
    cols = outs[0].shape[1]
    first = pl.multiple_of(tp_of(here_ref) * cols, cols)
    wide = rows_ref[...].astype(F32)
    scale = lax.rsqrt(jnp.mean(wide * wide, axis=-1, keepdims=True) + EPS)
    part = rows_ref[:, pl.ds(first, cols)].astype(F32)
    normed = (part * scale * gain_ref[:, pl.ds(first, cols)]).astype(BF16)
    numbers = lax.broadcasted_iota(jnp.int32, (experts, rows), 0)
    named = (ids_ref[0:1, :] == numbers) | (ids_ref[1:2, :] == numbers)
    before = (
        lax.broadcasted_iota(jnp.int32, (rows, rows), 0)
        < lax.broadcasted_iota(jnp.int32, (rows, rows), 1)
    ).astype(F32).astype(BF16)
    rank = jnp.dot(named.astype(F32).astype(BF16), before, preferred_element_type=F32)
    rank_ref[...] = jnp.where(named, rank, -1.0)
    slot = lax.broadcasted_iota(jnp.int32, (capacity, rows), 0).astype(F32)
    for k in range(experts):
        e = ep_of(here_ref) ^ k if len(outs) > 1 else k
        onehot_ref[k * capacity : (k + 1) * capacity, :] = (
            rank_ref[pl.ds(e, 1), :] == slot
        ).astype(F32)
    count = onehot_ref.shape[0] // len(outs)
    for k, out_ref in enumerate(outs):
        out_ref[...] = jnp.dot(
            onehot_ref[k * count : (k + 1) * count, :].astype(BF16),
            normed,
            preferred_element_type=F32,
        ).astype(BF16)


def dispatched(here, expert_input, norm_gain, ids_across, capacity, pieces):
    rows, width = expert_input.shape
    experts = lax.axis_size("ep")
    cols = width // lax.axis_size("tp")
    slots = experts * capacity
    return pl.pallas_call(
        functools.partial(dispatch_kernel, experts, capacity),
        out_shape=[jax.ShapeDtypeStruct((slots // pieces, cols), BF16)] * pieces,
        in_specs=[SMEM, VMEM, VMEM, VMEM],
        out_specs=[VMEM] * pieces,
        scratch_shapes=[pltpu.VMEM((slots, rows), F32), pltpu.VMEM((experts, rows), F32)],
        cost_estimate=pl.CostEstimate(
            flops=2 * slots * rows * cols, bytes_accessed=2 * rows * width, transcendentals=rows
        ),
        name="dispatch",
    )(here, ids_across, expert_input, norm_gain.reshape(1, width))


def arrange_kernel(here_ref, *refs):
    out_ref = refs[-1]
    for k, ref in enumerate(refs[:-1]):
        out_ref[half(ep_of(here_ref) ^ k, ref.shape[0]), :] = ref[...]


def fetch_kernel(gate, up, down, gate_w, up_w, down_w, sem):
    copies = []
    for n, (source, target) in enumerate(((gate, gate_w), (up, up_w), (down, down_w))):
        part = target.shape[0] // 4
        for k in range(4):
            rows = slice(k * part, (k + 1) * part)
            copies.append(
                pltpu.make_async_copy(source.at[0, rows, :], target.at[rows, :], sem.at[4 * n + k])
            )
    for copy in copies:
        copy.start()
    for copy in copies:
        copy.wait()


def fetched(*weights):
    hbm = pl.BlockSpec(memory_space=pltpu.HBM)
    vmem = pl.BlockSpec(memory_space=pltpu.VMEM)
    return pl.pallas_call(
        fetch_kernel,
        in_specs=[hbm] * 3,
        out_specs=[vmem] * 3,
        out_shape=[pltpu.VMEM(w.shape[1:], w.dtype) for w in weights],
        scratch_shapes=[pltpu.SemaphoreType.DMA((12,))],
        compiler_params=pltpu.CompilerParams(vmem_limit_bytes=4 * 1024 * 1024),
        cost_estimate=pl.CostEstimate(
            flops=sum(w.size for w in weights) * 100,
            bytes_accessed=sum(w.size for w in weights) * 2,
            transcendentals=0,
        ),
        name="fetch",
    )(*(pltpu.with_memory_space_constraint(w, pltpu.HBM) for w in weights))


def ffn_kernel(
    index, order_ref, own, near, far, cross, gate_w, up_w, down_w, keep_ref, send_ref
):
    rows, cols = far.shape
    mine = pl.ds(pl.multiple_of(order_ref[8 + index], rows), rows)
    pieces = (own[mine, :], near[mine, :], far[...], cross[...])

    def part(k):
        return pl.ds(pl.multiple_of(order_ref[k] * cols, cols), cols)

    def product(weight_w):
        return functools.reduce(
            jnp.add,
            [
                jnp.dot(piece, weight_w[part(k), :], preferred_element_type=F32)
                for k, piece in enumerate(pieces)
            ],
        )

    gate_act = product(gate_w)
    up_act = product(up_w)
    hidden = (gate_act / (1.0 + jnp.exp(-gate_act)) * up_act).astype(BF16)
    for n, out_ref in enumerate((send_ref, keep_ref)):
        for k in range(2):
            out_ref[:, k * cols : (k + 1) * cols] = jnp.dot(
                hidden, down_w[:, part(4 + 2 * n + k)], preferred_element_type=F32
            ).astype(BF16)


def ffn(order, index, own, near, far, cross, weights):
    rows, cols = far.shape
    width, units = weights[0].shape
    vmem = pl.BlockSpec(memory_space=pltpu.VMEM)
    return pl.pallas_call(
        functools.partial(ffn_kernel, index),
        in_specs=[pl.BlockSpec(memory_space=pltpu.SMEM)] + [vmem] * 7,
        out_specs=[vmem, vmem],
        out_shape=[jax.ShapeDtypeStruct((rows, 2 * cols), BF16)] * 2,
        compiler_params=pltpu.CompilerParams(vmem_limit_bytes=16 * 1024 * 1024),
        cost_estimate=pl.CostEstimate(
            flops=6 * rows * width * units,
            bytes_accessed=6 * width * units + 4 * rows * width,
            transcendentals=rows * units,
        ),
        name="ffn",
    )(
        order,
        own,
        near,
        far,
        cross,
        *(pltpu.with_memory_space_constraint(w, pltpu.VMEM) for w in weights),
    )


def total_kernel(here_ref, keep_ref, got_ref, over_ref, *rest):
    outs, part = rest[:-1], rest[-1]
    cols = over_ref.shape[1]
    capacity = outs[0].shape[0]
    part[...] = (
        keep_ref[:, :cols].astype(F32) + got_ref[:, :cols].astype(F32) + over_ref[...].astype(F32)
    )
    mine = lax.rem(ep_of(here_ref), len(outs))
    for k, out_ref in enumerate(outs):
        out_ref[...] = part[half(mine ^ k, capacity), :].astype(BF16)


def mix_kernel(weight_ref, *rest):
    pieces, out_ref, held = rest[:-2], rest[-2], rest[-1]
    count = pieces[0].shape[0]
    for k, piece in enumerate(pieces):
        held[k * count : (k + 1) * count, :] = piece[...]
    left = weight_ref[...]
    sums = None
    for _ in range(3):
        high = left.astype(BF16)
        left = left - high.astype(F32)
        one = lax.dot_general(
            high, held[...], (((0,), (0,)), ((), ())), preferred_element_type=F32
        )
        sums = one if sums is None else sums + one
    out_ref[...] = sums.astype(BF16)


def combine_weights(ids_across, weight_across, capacity, numbers):
    experts = numbers.shape[0]
    rows = ids_across.shape[1]
    numbers = numbers[:, None]
    first = ids_across[0:1] == numbers
    second = ids_across[1:2] == numbers
    named = first | second
    before = jnp.triu(jnp.ones((rows, rows), BF16), 1)
    rank = jnp.dot(named.astype(BF16), before, preferred_element_type=F32)
    weight = jnp.where(first, weight_across[0:1], 0.0) + jnp.where(second, weight_across[1:2], 0.0)
    slot = jnp.arange(capacity, dtype=jnp.int32).astype(F32)[None, :, None]
    held = (rank[:, None, :] == slot) & named[:, None, :]
    return jnp.where(held, weight[:, None, :], 0.0).reshape(experts * capacity, rows)


def shards(
    queries,
    key_rows,
    value_rows,
    head_lambda,
    sub_gain,
    out_weight,
    expert_input,
    norm_gain,
    route_ids,
    route_weight,
    gate_weight,
    up_weight,
    down_weight,
):
    rows_b, width = expert_input.shape
    experts = lax.axis_size("ep")
    capacity = 5 * route_ids.shape[1] * rows_b // (3 * experts)
    slots = experts * capacity
    place = lax.axis_index("tp").astype(jnp.int32)
    cols = width // lax.axis_size("tp")
    ids_across = route_ids.T
    weight_across = route_weight.T

    weights = fetched(gate_weight, up_weight, down_weight)
    small = experts <= 8 and experts & (experts - 1) == 0 and head_lambda.shape[0] == 2
    here = lax.axis_index("ep") * lax.axis_size("tp") + lax.axis_index("tp")
    here = here.astype(jnp.int32).reshape(1)
    outgoing = dispatched(
        here, expert_input, norm_gain, ids_across, capacity, experts if small else 1
    )
    if small:
        arrived = [outgoing[0]] + [swap(outgoing[k], "ep", k) for k in range(1, experts)]
        (own,) = local(arrange_kernel, [(slots, cols)], (here, *arrived))
    else:
        own = lax.all_to_all(
            outgoing[0].reshape(experts, capacity, cols), "ep", 0, 0, tiled=True
        ).reshape(slots, cols)
    if small:
        rows_a, deep = queries.shape[0], value_rows.shape[1] // 2
        pair = queries.shape[1] // 2
        trio = (queries, key_rows, value_rows)
        (picked,) = local(pick_kernel, [(rows_a, 2 * pair + deep)], (here, *trio), far=3)
        got = swap(picked, "ep", 1)
        query, block = local(
            merge_kernel, [(2 * rows_a, pair), (2 * rows_a, pair + deep)], (here, *trio, got), far=3
        )
    near = swap(own, "tp", 1)
    halves = 2
    part = slots // halves
    at = lax.axis_index("ep").astype(jnp.int32)
    side = at // (experts // 2)
    firsts = [(1 - side) * part, side * part]
    order = jnp.concatenate(
        [jnp.array([0, 1, 2, 3, 1, 3, 0, 2], jnp.int32) ^ place, jnp.stack(firsts)]
    )
    fars = [swap(lax.dynamic_slice_in_dim(own, first, part), "tp", 2) for first in firsts]
    if small:
        blocks = []
        for k in range(1, experts // 2):
            moving = blocks[k - 3] if k > 2 else block
            blocks.append(onward(moving, "ep", 2 * min(k, 2), 2 * max(k - 2, 0)))
    mine, gots = [], []
    for i in range(halves):
        cross = swap(fars[i], "tp", 1)
        keep, send = ffn(order, i, own, near, fars[i], cross, weights)
        got = swap(send, "tp", 1)
        across = (keep[:, cols:].astype(F32) + got[:, cols:].astype(F32)).astype(BF16)
        gots.append(swap(across, "tp", 2))
        mine.append((keep, got))
    if small:
        kept, sent = local(
            functools.partial(attention_kernel, pair // 2),
            [(rows_a, deep)] * 2,
            (here, head_lambda, query, block, *blocks, sub_gain.reshape(1, -1)),
            smem=2,
            scratch=[pltpu.VMEM((2 * rows_a, deep), BF16)],
            flops=16 * rows_a * rows_a * experts * pair,
            limit=20,
        )
        got = swap(sent, "ep", 1)
        model = out_weight.shape[1]
        kept, sent = local(
            project_kernel,
            [(rows_a // 2, model)] * 2,
            (here, kept, got, out_weight),
            scratch=[pltpu.VMEM((rows_a, 2 * deep), BF16)],
            flops=4 * rows_a * deep * model,
        )
        got = swap(sent, "tp", 1)
        group = got.shape[0] // 2
        across = (kept[group:].astype(F32) + got[group:].astype(F32)).astype(BF16)
        last = swap(across, "tp", 2)
        mixer_out = (
            kept[:group].astype(F32) + got[:group].astype(F32) + last.astype(F32)
        ).astype(BF16)
    else:
        key_rows, value_rows, _ = lax.optimization_barrier((key_rows, value_rows, own))
        both, places = gathered_keys(key_rows, value_rows)
        share = attention(queries, both, places, head_lambda, sub_gain, out_weight)
        parts = lax.all_to_all(
            share.reshape(lax.axis_size("tp"), -1, share.shape[1]), "tp", 0, 0, tiled=True
        )
        mixer_out = jnp.sum(parts.astype(F32), axis=0).astype(BF16)
    steps = jnp.arange(experts, dtype=jnp.int32)
    if not small:
        summed = jnp.zeros((slots, cols), BF16)
        for (keep, got), over, first in zip(mine, gots, firsts):
            one = keep[:, :cols].astype(F32) + got[:, :cols].astype(F32) + over.astype(F32)
            summed = lax.dynamic_update_slice_in_dim(summed, one.astype(BF16), first, 0)
        returned = lax.all_to_all(
            summed.reshape(experts, capacity, cols), "ep", split_axis=0, concat_axis=0, tiled=True
        ).reshape(slots, cols)
        mixed = lax.dot_general(
            combine_weights(ids_across, weight_across, capacity, steps),
            returned.astype(F32),
            (((0,), (0,)), ((), ())),
            precision=lax.Precision.HIGHEST,
            preferred_element_type=F32,
        )
        return (mixer_out, mixed.astype(BF16))
    count = experts // 2
    pieces = [None] * experts
    for i, ((keep, got), over) in enumerate(zip(mine, gots)):
        outs = local(
            total_kernel,
            [(capacity, cols)] * count,
            (here, keep, got, over),
            scratch=[pltpu.VMEM((part, cols), F32)],
        )
        for k, piece in enumerate(outs):
            k += (1 - i) * count
            pieces[k] = swap(piece, "ep", k) if k else piece
    (mixed,) = local(
        mix_kernel,
        [(rows_b, cols)],
        (combine_weights(ids_across, weight_across, capacity, at ^ steps), *pieces),
        smem=0,
        scratch=[pltpu.VMEM((slots, cols), BF16)],
        flops=6 * slots * rows_b * cols,
    )
    return (mixer_out, mixed)


def solution(mesh):
    placed = (
        P("ep", "tp"),
        P("ep", "tp"),
        P("ep", "tp"),
        P("tp"),
        P(),
        P("tp", None),
        P("ep", None),
        P(),
        P("ep", None),
        P("ep", None),
        P("ep", None, "tp"),
        P("ep", None, "tp"),
        P("ep", "tp", None),
    )

    return jax.shard_map(
        shards,
        mesh=mesh,
        in_specs=placed,
        out_specs=(P(("ep", "tp"), None), P("ep", "tp")),
        check_vma=False,
    )
```

```python
import functools

import jax
import jax.numpy as jnp
from jax import lax
from jax.experimental import pallas as pl
from jax.experimental.pallas import tpu as pltpu
from jax.sharding import PartitionSpec as P

EPS = 1e-06
F32 = jnp.float32
BF16 = jnp.bfloat16


def swap(x, axis, mask):
    count = lax.axis_size(axis)
    return lax.ppermute(x, axis, [(i, i ^ mask) for i in range(count)])


def ep_of(here_ref):
    return lax.div(here_ref[0], lax.axis_size("tp"))


def tp_of(here_ref):
    return lax.rem(here_ref[0], lax.axis_size("tp"))


def onward(x, axis, step, first):
    count = lax.axis_size(axis)
    return lax.ppermute(x, axis, [(i, i + step) for i in range(first, count - step)])


def gathered_keys(key_rows, value_rows):
    count = lax.axis_size("ep")
    own = jnp.concatenate([key_rows, value_rows], axis=1)
    both = lax.all_gather(own, "ep", axis=0, tiled=True)
    return both, jnp.arange(count, dtype=jnp.int32)


def attention(queries, both, places, head_lambda, sub_gain, out_weight):
    rows_here = queries.shape[0]
    heads_here = head_lambda.shape[0]
    head_width = queries.shape[1] // (2 * heads_here)
    width = queries.shape[1]
    value_width = (both.shape[1] - width) // heads_here
    scaling = head_width ** (-0.5)
    length = both.shape[0]
    query_blocks = queries.reshape(rows_here, heads_here, 2, head_width)
    query_pos = lax.axis_index("ep") * rows_here + jnp.arange(rows_here, dtype=jnp.int32)
    key_pos = (
        places[:, None] * rows_here + jnp.arange(rows_here, dtype=jnp.int32)[None, :]
    ).reshape(length)
    key_blocks = both[:, :width].reshape(length, heads_here, 2, head_width)
    value_blocks = both[:, width:].reshape(length, heads_here, value_width)
    scores = (
        jnp.einsum("qhmd,khmd->hmqk", query_blocks, key_blocks, preferred_element_type=F32)
        * scaling
    )
    allowed = (query_pos[:, None] >= key_pos[None, :]) & (key_pos[None, :] >= 0)
    scores = jnp.where(allowed, scores, -1e30)
    row_max = jnp.max(scores, axis=-1)
    weights = jnp.where(allowed, jnp.exp(scores - row_max[..., None]), 0.0)
    row_total = jnp.sum(weights, axis=-1)
    numerator = jnp.einsum(
        "hmqk,khd->hmqd", weights.astype(BF16), value_blocks, preferred_element_type=F32
    )
    per_map = numerator / row_total[..., None]
    contrast = per_map[:, 0] - head_lambda[:, None, None] * per_map[:, 1]
    normed = (
        contrast * lax.rsqrt(jnp.mean(contrast * contrast, axis=-1, keepdims=True) + EPS) * sub_gain
    ).astype(BF16)
    attended = jnp.transpose(normed, (1, 0, 2)).reshape(rows_here, heads_here * value_width)
    return jnp.dot(attended, out_weight, preferred_element_type=F32).astype(BF16)


VMEM = pl.BlockSpec(memory_space=pltpu.VMEM)
SMEM = pl.BlockSpec(memory_space=pltpu.SMEM)


def half(index, size):
    return pl.ds(pl.multiple_of(index * size, size), size)


def pick_kernel(place_ref, query_ref, key_ref, value_ref, out_ref):
    other = 1 - (ep_of(place_ref) & 1)
    at = 0
    for ref in (query_ref, key_ref, value_ref):
        wide = ref.shape[1] // 2
        out_ref[:, at : at + wide] = ref[:, half(other, wide)]
        at += wide


def merge_kernel(place_ref, query_ref, key_ref, value_ref, got_ref, query_out, block_out):
    mine = ep_of(place_ref) & 1
    rows = query_ref.shape[0]
    pair, deep = key_ref.shape[1] // 2, value_ref.shape[1] // 2
    own, other = half(mine, rows), half(1 - mine, rows)
    query_out[own, :] = query_ref[:, half(mine, pair)]
    query_out[other, :] = got_ref[:, :pair]
    block_out[own, :pair] = key_ref[:, half(mine, pair)]
    block_out[own, pair:] = value_ref[:, half(mine, deep)]
    block_out[other, :] = got_ref[:, pair:]


def attention_kernel(head_width, place_ref, lambda_ref, query_ref, own_ref, *rest):
    lines = rest[:-4]
    gain_ref, keep_ref, send_ref, attended = rest[-4:]
    rows = query_ref.shape[0] // 2
    pair = 2 * head_width
    mine, line_place = ep_of(place_ref) & 1, ep_of(place_ref) >> 1
    causal = lax.broadcasted_iota(jnp.int32, (rows, rows), 0) >= lax.broadcasted_iota(
        jnp.int32, (rows, rows), 1
    )
    lane = lax.broadcasted_iota(jnp.int32, (rows, pair), 1)
    scaling = head_width ** (-0.5)
    lam = lambda_ref[mine]
    for side in range(2):
        query = query_ref[side * rows : (side + 1) * rows, :].astype(F32)
        pieces = [(own_ref, side * rows, rows, None)]
        if side:
            pieces.append((own_ref, 0, rows, 0.0))
        for k, ref in enumerate(lines):
            bias = jnp.where(line_place >= k + 1, 0.0, -1e30).astype(F32)
            pieces += [(ref, 0, rows, bias), (ref, rows, rows, bias)]
        per_map = []
        for m in range(2):
            one = jnp.where(lane // head_width == m, query, 0.0).astype(BF16)
            scores = []
            for ref, first, count, bias in pieces:
                s = scaling * lax.dot_general(
                    one,
                    ref[first : first + count, :pair],
                    (((1,), (1,)), ((), ())),
                    preferred_element_type=F32,
                )
                scores.append(jnp.where(causal, s, -1e30) if bias is None else s + bias)
            top = jnp.max(functools.reduce(jnp.maximum, scores), axis=-1, keepdims=True)
            weights = [jnp.exp(s - top) for s in scores]
            row_sum = jnp.sum(functools.reduce(jnp.add, weights), axis=-1, keepdims=True)
            numerator = functools.reduce(
                jnp.add,
                [
                    jnp.dot(
                        w.astype(BF16),
                        ref[first : first + count, pair:],
                        preferred_element_type=F32,
                    )
                    for w, (ref, first, count, _) in zip(weights, pieces)
                ],
            )
            per_map.append(numerator / row_sum)
        contrast = per_map[0] - lam * per_map[1]
        square = jnp.mean(contrast * contrast, axis=-1, keepdims=True)
        attended[side * rows : (side + 1) * rows, :] = (
            contrast * lax.rsqrt(square + EPS) * gain_ref[...]
        ).astype(BF16)
    keep_ref[...] = attended[half(mine, rows), :]
    send_ref[...] = attended[half(1 - mine, rows), :]


def project_kernel(place_ref, own_ref, got_ref, weight_ref, keep_ref, send_ref, attended):
    mine, place = ep_of(place_ref) & 1, tp_of(place_ref)
    rows, deep = own_ref.shape
    attended[:, half(mine, deep)] = own_ref[...]
    attended[:, half(1 - mine, deep)] = got_ref[...]
    group = rows // 4
    for out_ref, masks in ((send_ref, (1, 3)), (keep_ref, (0, 2))):
        picked = [attended[half(place ^ mask, group), :] for mask in masks]
        out_ref[...] = jnp.dot(
            jnp.concatenate(picked, axis=0), weight_ref[...], preferred_element_type=F32
        ).astype(BF16)


def close_kernel(keep_ref, got_ref, last_ref, out_ref):
    rows = last_ref.shape[0]
    out_ref[...] = (
        keep_ref[:rows, :].astype(F32) + got_ref[:rows, :].astype(F32) + last_ref[...].astype(F32)
    ).astype(BF16)


def local(kernel, outs, operands, smem=1, scratch=(), flops=1000000, limit=12, far=0):
    size = sum(x.size for x in operands)
    operands = list(operands)
    specs, options = [VMEM] * (len(operands) - smem), {}
    outs_specs = [VMEM] * len(outs)
    if far:
        for n in range(smem, smem + far):
            operands[n] = pltpu.with_memory_space_constraint(operands[n], pltpu.HBM)
        whole = lambda i: (0, 0)
        options["grid"] = (1,)
        specs = [pl.BlockSpec(x.shape, whole) for x in operands[smem:]]
        outs_specs = [pl.BlockSpec(shape, whole) for shape in outs]
    return pl.pallas_call(
        kernel,
        out_shape=[jax.ShapeDtypeStruct(shape, BF16) for shape in outs],
        in_specs=[SMEM] * smem + specs,
        out_specs=outs_specs,
        **options,
        scratch_shapes=list(scratch),
        compiler_params=pltpu.CompilerParams(vmem_limit_bytes=limit * 1024 * 1024),
        cost_estimate=pl.CostEstimate(
            flops=flops, bytes_accessed=2 * size, transcendentals=0
        ),
    )(*operands)


def dispatch_kernel(experts, capacity, here_ref, ids_ref, rows_ref, gain_ref, *rest):
    outs, onehot_ref, rank_ref = rest[:-2], rest[-2], rest[-1]
    rows, _ = rows_ref.shape
    cols = outs[0].shape[1]
    first = pl.multiple_of(tp_of(here_ref) * cols, cols)
    wide = rows_ref[...].astype(F32)
    scale = lax.rsqrt(jnp.mean(wide * wide, axis=-1, keepdims=True) + EPS)
    part = rows_ref[:, pl.ds(first, cols)].astype(F32)
    normed = (part * scale * gain_ref[:, pl.ds(first, cols)]).astype(BF16)
    numbers = lax.broadcasted_iota(jnp.int32, (experts, rows), 0)
    named = (ids_ref[0:1, :] == numbers) | (ids_ref[1:2, :] == numbers)
    before = (
        lax.broadcasted_iota(jnp.int32, (rows, rows), 0)
        < lax.broadcasted_iota(jnp.int32, (rows, rows), 1)
    ).astype(F32).astype(BF16)
    rank = jnp.dot(named.astype(F32).astype(BF16), before, preferred_element_type=F32)
    rank_ref[...] = jnp.where(named, rank, -1.0)
    slot = lax.broadcasted_iota(jnp.int32, (capacity, rows), 0).astype(F32)
    for k in range(experts):
        e = ep_of(here_ref) ^ k if len(outs) > 1 else k
        onehot_ref[k * capacity : (k + 1) * capacity, :] = (
            rank_ref[pl.ds(e, 1), :] == slot
        ).astype(F32)
    count = onehot_ref.shape[0] // len(outs)
    for k, out_ref in enumerate(outs):
        out_ref[...] = jnp.dot(
            onehot_ref[k * count : (k + 1) * count, :].astype(BF16),
            normed,
            preferred_element_type=F32,
        ).astype(BF16)


def dispatched(here, expert_input, norm_gain, ids_across, capacity, pieces):
    rows, width = expert_input.shape
    experts = lax.axis_size("ep")
    cols = width // lax.axis_size("tp")
    slots = experts * capacity
    return pl.pallas_call(
        functools.partial(dispatch_kernel, experts, capacity),
        out_shape=[jax.ShapeDtypeStruct((slots // pieces, cols), BF16)] * pieces,
        in_specs=[SMEM, VMEM, VMEM, VMEM],
        out_specs=[VMEM] * pieces,
        scratch_shapes=[pltpu.VMEM((slots, rows), F32), pltpu.VMEM((experts, rows), F32)],
        cost_estimate=pl.CostEstimate(
            flops=2 * slots * rows * cols, bytes_accessed=2 * rows * width, transcendentals=rows
        ),
        name="dispatch",
    )(here, ids_across, expert_input, norm_gain.reshape(1, width))


def arrange_kernel(here_ref, *refs):
    out_ref = refs[-1]
    for k, ref in enumerate(refs[:-1]):
        out_ref[half(ep_of(here_ref) ^ k, ref.shape[0]), :] = ref[...]


def fetch_kernel(gate, up, down, gate_w, up_w, down_w, sem):
    copies = []
    for n, (source, target) in enumerate(((gate, gate_w), (up, up_w), (down, down_w))):
        part = target.shape[0] // 4
        for k in range(4):
            rows = slice(k * part, (k + 1) * part)
            copies.append(
                pltpu.make_async_copy(source.at[0, rows, :], target.at[rows, :], sem.at[4 * n + k])
            )
    for copy in copies:
        copy.start()
    for copy in copies:
        copy.wait()


def fetched(*weights):
    hbm = pl.BlockSpec(memory_space=pltpu.HBM)
    vmem = pl.BlockSpec(memory_space=pltpu.VMEM)
    return pl.pallas_call(
        fetch_kernel,
        in_specs=[hbm] * 3,
        out_specs=[vmem] * 3,
        out_shape=[pltpu.VMEM(w.shape[1:], w.dtype) for w in weights],
        scratch_shapes=[pltpu.SemaphoreType.DMA((12,))],
        compiler_params=pltpu.CompilerParams(vmem_limit_bytes=4 * 1024 * 1024),
        cost_estimate=pl.CostEstimate(
            flops=sum(w.size for w in weights) * 100,
            bytes_accessed=sum(w.size for w in weights) * 2,
            transcendentals=0,
        ),
        name="fetch",
    )(*(pltpu.with_memory_space_constraint(w, pltpu.HBM) for w in weights))


def ffn_kernel(
    index, order_ref, own, near, far, cross, gate_w, up_w, down_w, keep_ref, send_ref
):
    rows, cols = far.shape
    mine = pl.ds(pl.multiple_of(order_ref[8 + index], rows), rows)
    pieces = (own[mine, :], near[mine, :], far[...], cross[...])

    def part(k):
        return pl.ds(pl.multiple_of(order_ref[k] * cols, cols), cols)

    def product(weight_w):
        return functools.reduce(
            jnp.add,
            [
                jnp.dot(piece, weight_w[part(k), :], preferred_element_type=F32)
                for k, piece in enumerate(pieces)
            ],
        )

    gate_act = product(gate_w)
    up_act = product(up_w)
    hidden = (gate_act / (1.0 + jnp.exp(-gate_act)) * up_act).astype(BF16)
    for n, out_ref in enumerate((send_ref, keep_ref)):
        for k in range(2):
            out_ref[:, k * cols : (k + 1) * cols] = jnp.dot(
                hidden, down_w[:, part(4 + 2 * n + k)], preferred_element_type=F32
            ).astype(BF16)


def ffn(order, index, own, near, far, cross, weights):
    rows, cols = far.shape
    width, units = weights[0].shape
    vmem = pl.BlockSpec(memory_space=pltpu.VMEM)
    return pl.pallas_call(
        functools.partial(ffn_kernel, index),
        in_specs=[pl.BlockSpec(memory_space=pltpu.SMEM)] + [vmem] * 7,
        out_specs=[vmem, vmem],
        out_shape=[jax.ShapeDtypeStruct((rows, 2 * cols), BF16)] * 2,
        compiler_params=pltpu.CompilerParams(vmem_limit_bytes=16 * 1024 * 1024),
        cost_estimate=pl.CostEstimate(
            flops=6 * rows * width * units,
            bytes_accessed=6 * width * units + 4 * rows * width,
            transcendentals=rows * units,
        ),
        name="ffn",
    )(
        order,
        own,
        near,
        far,
        cross,
        *(pltpu.with_memory_space_constraint(w, pltpu.VMEM) for w in weights),
    )


def total_kernel(here_ref, keep_ref, got_ref, over_ref, *rest):
    outs, part = rest[:-1], rest[-1]
    cols = over_ref.shape[1]
    capacity = outs[0].shape[0]
    part[...] = (
        keep_ref[:, :cols].astype(F32) + got_ref[:, :cols].astype(F32) + over_ref[...].astype(F32)
    )
    mine = lax.rem(ep_of(here_ref), len(outs))
    for k, out_ref in enumerate(outs):
        out_ref[...] = part[half(mine ^ k, capacity), :].astype(BF16)


def mix_kernel(weight_ref, *rest):
    pieces, out_ref, held = rest[:-2], rest[-2], rest[-1]
    count = pieces[0].shape[0]
    for k, piece in enumerate(pieces):
        held[k * count : (k + 1) * count, :] = piece[...]
    left = weight_ref[...]
    sums = None
    for _ in range(3):
        high = left.astype(BF16)
        left = left - high.astype(F32)
        one = lax.dot_general(
            high, held[...], (((0,), (0,)), ((), ())), preferred_element_type=F32
        )
        sums = one if sums is None else sums + one
    out_ref[...] = sums.astype(BF16)


def combine_weights(ids_across, weight_across, capacity, numbers):
    experts = numbers.shape[0]
    rows = ids_across.shape[1]
    numbers = numbers[:, None]
    first = ids_across[0:1] == numbers
    second = ids_across[1:2] == numbers
    named = first | second
    before = jnp.triu(jnp.ones((rows, rows), BF16), 1)
    rank = jnp.dot(named.astype(BF16), before, preferred_element_type=F32)
    weight = jnp.where(first, weight_across[0:1], 0.0) + jnp.where(second, weight_across[1:2], 0.0)
    slot = jnp.arange(capacity, dtype=jnp.int32).astype(F32)[None, :, None]
    held = (rank[:, None, :] == slot) & named[:, None, :]
    return jnp.where(held, weight[:, None, :], 0.0).reshape(experts * capacity, rows)


def shards(
    queries,
    key_rows,
    value_rows,
    head_lambda,
    sub_gain,
    out_weight,
    expert_input,
    norm_gain,
    route_ids,
    route_weight,
    gate_weight,
    up_weight,
    down_weight,
):
    rows_b, width = expert_input.shape
    experts = lax.axis_size("ep")
    capacity = 5 * route_ids.shape[1] * rows_b // (3 * experts)
    slots = experts * capacity
    place = lax.axis_index("tp").astype(jnp.int32)
    cols = width // lax.axis_size("tp")
    ids_across = route_ids.T
    weight_across = route_weight.T

    weights = fetched(gate_weight, up_weight, down_weight)
    small = experts <= 8 and experts & (experts - 1) == 0 and head_lambda.shape[0] == 2
    here = lax.axis_index("ep") * lax.axis_size("tp") + lax.axis_index("tp")
    here = here.astype(jnp.int32).reshape(1)
    outgoing = dispatched(
        here, expert_input, norm_gain, ids_across, capacity, experts if small else 1
    )
    if small:
        arrived = [outgoing[0]] + [swap(outgoing[k], "ep", k) for k in range(1, experts)]
        (own,) = local(arrange_kernel, [(slots, cols)], (here, *arrived))
    else:
        own = lax.all_to_all(
            outgoing[0].reshape(experts, capacity, cols), "ep", 0, 0, tiled=True
        ).reshape(slots, cols)
    if small:
        rows_a, deep = queries.shape[0], value_rows.shape[1] // 2
        pair = queries.shape[1] // 2
        trio = (queries, key_rows, value_rows)
        (picked,) = local(pick_kernel, [(rows_a, 2 * pair + deep)], (here, *trio), far=3)
        got = swap(picked, "ep", 1)
        query, block = local(
            merge_kernel, [(2 * rows_a, pair), (2 * rows_a, pair + deep)], (here, *trio, got), far=3
        )
    near = swap(own, "tp", 1)
    halves = 2
    part = slots // halves
    at = lax.axis_index("ep").astype(jnp.int32)
    side = at // (experts // 2)
    firsts = [(1 - side) * part, side * part]
    order = jnp.concatenate(
        [jnp.array([0, 1, 2, 3, 1, 3, 0, 2], jnp.int32) ^ place, jnp.stack(firsts)]
    )
    fars = [swap(lax.dynamic_slice_in_dim(own, first, part), "tp", 2) for first in firsts]
    if small:
        blocks = []
        for k in range(1, experts // 2):
            moving = blocks[k - 3] if k > 2 else block
            blocks.append(onward(moving, "ep", 2 * min(k, 2), 2 * max(k - 2, 0)))
    mine, gots = [], []
    for i in range(halves):
        cross = swap(fars[i], "tp", 1)
        keep, send = ffn(order, i, own, near, fars[i], cross, weights)
        got = swap(send, "tp", 1)
        across = (keep[:, cols:].astype(F32) + got[:, cols:].astype(F32)).astype(BF16)
        gots.append(swap(across, "tp", 2))
        mine.append((keep, got))
    if small:
        kept, sent = local(
            functools.partial(attention_kernel, pair // 2),
            [(rows_a, deep)] * 2,
            (here, head_lambda, query, block, *blocks, sub_gain.reshape(1, -1)),
            smem=2,
            scratch=[pltpu.VMEM((2 * rows_a, deep), BF16)],
            flops=16 * rows_a * rows_a * experts * pair,
            limit=20,
        )
        got = swap(sent, "ep", 1)
        model = out_weight.shape[1]
        kept, sent = local(
            project_kernel,
            [(rows_a // 2, model)] * 2,
            (here, kept, got, out_weight),
            scratch=[pltpu.VMEM((rows_a, 2 * deep), BF16)],
            flops=4 * rows_a * deep * model,
        )
        got = swap(sent, "tp", 1)
        group = got.shape[0] // 2
        across = (kept[group:].astype(F32) + got[group:].astype(F32)).astype(BF16)
        last = swap(across, "tp", 2)
        (mixer_out,) = local(close_kernel, [last.shape], (kept, got, last), smem=0)
    else:
        key_rows, value_rows, _ = lax.optimization_barrier((key_rows, value_rows, own))
        both, places = gathered_keys(key_rows, value_rows)
        share = attention(queries, both, places, head_lambda, sub_gain, out_weight)
        parts = lax.all_to_all(
            share.reshape(lax.axis_size("tp"), -1, share.shape[1]), "tp", 0, 0, tiled=True
        )
        mixer_out = jnp.sum(parts.astype(F32), axis=0).astype(BF16)
    steps = jnp.arange(experts, dtype=jnp.int32)
    if not small:
        summed = jnp.zeros((slots, cols), BF16)
        for (keep, got), over, first in zip(mine, gots, firsts):
            one = keep[:, :cols].astype(F32) + got[:, :cols].astype(F32) + over.astype(F32)
            summed = lax.dynamic_update_slice_in_dim(summed, one.astype(BF16), first, 0)
        returned = lax.all_to_all(
            summed.reshape(experts, capacity, cols), "ep", split_axis=0, concat_axis=0, tiled=True
        ).reshape(slots, cols)
        mixed = lax.dot_general(
            combine_weights(ids_across, weight_across, capacity, steps),
            returned.astype(F32),
            (((0,), (0,)), ((), ())),
            precision=lax.Precision.HIGHEST,
            preferred_element_type=F32,
        )
        return (mixer_out, mixed.astype(BF16))
    count = experts // 2
    pieces = [None] * experts
    for i, ((keep, got), over) in enumerate(zip(mine, gots)):
        outs = local(
            total_kernel,
            [(capacity, cols)] * count,
            (here, keep, got, over),
            scratch=[pltpu.VMEM((part, cols), F32)],
        )
        for k, piece in enumerate(outs):
            k += (1 - i) * count
            pieces[k] = swap(piece, "ep", k) if k else piece
    (mixed,) = local(
        mix_kernel,
        [(rows_b, cols)],
        (combine_weights(ids_across, weight_across, capacity, at ^ steps), *pieces),
        smem=0,
        scratch=[pltpu.VMEM((slots, cols), BF16)],
        flops=6 * slots * rows_b * cols,
    )
    return (mixer_out, mixed)


def solution(mesh):
    placed = (
        P("ep", "tp"),
        P("ep", "tp"),
        P("ep", "tp"),
        P("tp"),
        P(),
        P("tp", None),
        P("ep", None),
        P(),
        P("ep", None),
        P("ep", None),
        P("ep", None, "tp"),
        P("ep", None, "tp"),
        P("ep", "tp", None),
    )

    return jax.shard_map(
        shards,
        mesh=mesh,
        in_specs=placed,
        out_specs=(P(("ep", "tp"), None), P("ep", "tp")),
        check_vma=False,
    )
```
